32 devices in a mesh: rep: 2 (over x), fs: 8 (over z, y), tp: 2 (over core).
Axes of the slice: x: 2, y: 2, z: 4, core: 2. Of those that a mesh axis runs over, the one named last changes fastest.
Arguments:
- tokens: bfloat16 [8192, 2048], P(('rep', 'fs'), 'tp'), may hold values from -6 to 6
- mix_gain: float32 [2048], replicated, may hold values from 0.1 to 1.9
- query_w: bfloat16 [2048, 2048], P('fs', 'tp'), may hold values from -0.125 to 0.125
- key_w: bfloat16 [2048, 2048], P('fs', 'tp'), may hold values from -0.125 to 0.125
- value_w: bfloat16 [2048, 4096], P('fs', 'tp'), may hold values from -0.125 to 0.125
- head_gain: float32 [8, 512], replicated, may hold values from 0.1 to 1.9
- out_w: bfloat16 [4096, 2048], P('tp', 'fs'), may hold values from -0.09375 to 0.09375
- chan_gain: float32 [2048], replicated, may hold values from 0.1 to 1.9
- up_w: bfloat16 [2048, 4096], P('fs', 'tp'), may hold values from -0.125 to 0.125
- down_w: bfloat16 [4096, 2048], P('tp', 'fs'), may hold values from -0.09375 to 0.09375
Outputs:
- layer_out: bfloat16 [8192, 2048], P(('rep', 'fs'), 'tp')
The draws below stay inside these ranges and needn't reach their ends.
All inputs are finite; a program needn't handle non-finite values.
Results may differ from the reference program's by a relative error of at most 0.019.
Values may be sent and summed in bfloat16 or wider, within the bound.
A program may use at most 128 MiB of HBM per device.

```python
import jax
import jax.numpy as jnp
from jax import lax

D = 2048
HEADS = 8
DK = 256
DV = 512
FF = 4096
BLOCK = 128
TOK = 512
TOKENS = 8192
N_TP = 2


def block_scale(key, dims, shards, low, high):
    def one(dim, blocks):
        draws = jax.random.uniform(jax.random.fold_in(jax.random.fold_in(key, 6), dim), (blocks,), jnp.float32, low / len(shards), high / len(shards))
        return jnp.repeat(jnp.exp(draws), dims[dim] // blocks).reshape((-1,) + (1,) * (len(dims) - dim - 1))

    level = one(*shards[0])
    for cut in shards[1:]:
        level = level * one(*cut)
    return level


def noise(stream_key, shape, deviation, bound, shards=(), kind=jnp.bfloat16):
    values = jax.random.normal(stream_key, shape, jnp.float32) * deviation
    if len(shards) > 0:
        values = block_scale(stream_key, shape, shards, -0.22, 0.18) * values
    return jnp.clip(values, min=-bound, max=bound).astype(kind)


def setup_inputs(seed: int = 0) -> dict:
    splits = jax.random.split(jax.random.key(seed), 11)
    return {
        "tokens": noise(splits[0], (TOKENS, D), 1.0, 6.0, ((0, 16), (1, 2))),
        "mix_gain": jnp.clip(1.0 + 0.18 * jax.random.normal(splits[1], (D,), jnp.float32), 0.1, 1.9),
        "query_w": noise(splits[2], (D, D), D ** -0.5, 0.125, ((0, 8), (1, 2))),
        "key_w": noise(splits[3], (D, D), D ** -0.5, 0.125, ((0, 8), (1, 2))),
        "value_w": noise(splits[4], (D, HEADS * DV), D ** -0.5, 0.125, ((0, 8), (1, 2))),
        "head_gain": jnp.clip(1.0 + 0.18 * jax.random.normal(splits[5], (HEADS, DV), jnp.float32), 0.1, 1.9),
        "out_w": noise(splits[6], (HEADS * DV, D), (HEADS * DV) ** -0.5, 0.09375, ((0, 2), (1, 8))),
        "chan_gain": jnp.clip(1.0 + 0.18 * jax.random.normal(splits[7], (D,), jnp.float32), 0.1, 1.9),
        "up_w": noise(splits[8], (D, FF), D ** -0.5, 0.125, ((0, 8), (1, 2))),
        "down_w": noise(splits[9], (FF, D), FF ** -0.5, 0.09375, ((0, 2), (1, 8))),
    }


EPS = 1e-06
HEAD_EPS = 0.05
THETA = 10000.0

def norm_rows(rows, gain):
    values = rows.astype(jnp.float32)
    scale = lax.rsqrt(lax.optimization_barrier(jnp.mean(values * values, axis=-1, keepdims=True)) + EPS)
    return (values * scale * gain).astype(jnp.bfloat16)

def rotate(field, places):
    half = field.shape[-1] // 2
    inverse = THETA ** (-jnp.arange(half, dtype=jnp.float32) / half)
    angles = places[:, None] * inverse
    cosine = jnp.cos(angles)[:, None, :]
    sine = jnp.sin(angles)[:, None, :]
    first = field[..., :half]
    second = field[..., half:]
    return jnp.concatenate([first * cosine - second * sine, second * cosine + first * sine], axis=-1)

def retain(query, keys, values, log_rate):
    count = query.shape[0] // BLOCK
    q_blocks = query.reshape(count, BLOCK, query.shape[1])
    k_blocks = keys.reshape(count, BLOCK, keys.shape[1])
    v_blocks = values.reshape(count, BLOCK, values.shape[1])
    place = jnp.arange(BLOCK, dtype=jnp.float32)
    offset = place[:, None] - place[None, :]
    mask = jnp.where(offset >= 0, jnp.exp(log_rate * jnp.maximum(offset, 0.0)), 0.0)
    q_decay = jnp.exp(log_rate * (place + 1.0))
    k_decay = jnp.exp(log_rate * (BLOCK - 1.0 - place))
    block_decay = jnp.exp(log_rate * BLOCK)

    def advance(state, item):
        q_part, k_part, v_part = item
        scores = jnp.dot(q_part, k_part.T, preferred_element_type=jnp.float32)
        weights = (scores * mask).astype(jnp.bfloat16)
        result = jnp.dot(weights, v_part, preferred_element_type=jnp.float32)
        q_scaled = (q_part.astype(jnp.float32) * q_decay[:, None]).astype(jnp.bfloat16)
        result = result + jnp.dot(q_scaled, state.astype(jnp.bfloat16), preferred_element_type=jnp.float32)
        k_scaled = (k_part.astype(jnp.float32) * k_decay[:, None]).astype(jnp.bfloat16)
        state = state * block_decay + jnp.dot(k_scaled.T, v_part, preferred_element_type=jnp.float32)
        return (state, result)
    start = jnp.zeros((query.shape[1], values.shape[1]), jnp.float32)
    _, outputs = lax.scan(advance, start, (q_blocks, k_blocks, v_blocks))
    return outputs.reshape(count * BLOCK, values.shape[1])

def grouped_sum(left, right):
    width = left.shape[1] // N_TP
    total = jnp.zeros((left.shape[0], right.shape[1]), jnp.float32)
    for group in range(N_TP):
        term = jnp.dot(left[:, group * width:(group + 1) * width], right[group * width:(group + 1) * width], preferred_element_type=jnp.float32).astype(jnp.bfloat16)
        term = lax.optimization_barrier(term)
        total = total + term.astype(jnp.float32)
    return total

def reference(tokens, mix_gain, query_w, key_w, value_w, head_gain, out_w, chan_gain, up_w, down_w):
    normed = norm_rows(tokens, mix_gain)
    qraw = jnp.dot(normed, query_w, preferred_element_type=jnp.float32)
    kraw = jnp.dot(normed, key_w, preferred_element_type=jnp.float32)
    vraw = jnp.dot(normed, value_w, preferred_element_type=jnp.float32)
    places = (jnp.arange(TOKENS, dtype=jnp.int32) % TOK).astype(jnp.float32)
    query = rotate(qraw.reshape(TOKENS, HEADS, DK), places).astype(jnp.bfloat16)
    keys = (rotate(kraw.reshape(TOKENS, HEADS, DK), places) * DK ** (-0.5)).astype(jnp.bfloat16)
    values = vraw.reshape(TOKENS, HEADS, DV).astype(jnp.bfloat16)
    heads = jnp.arange(HEADS, dtype=jnp.int32).astype(jnp.float32)
    log_rate = jnp.log1p(-jnp.exp2(-5.0 - heads))
    count = TOKENS // TOK
    per_head = jax.vmap(retain, in_axes=(1, 1, 1, 0), out_axes=1)

    def one_sequence(item):
        return per_head(item[0], item[1], item[2], log_rate)
    retained = lax.map(one_sequence, (query.reshape(count, TOK, HEADS, DK), keys.reshape(count, TOK, HEADS, DK), values.reshape(count, TOK, HEADS, DV)))
    retained = retained.reshape(TOKENS, HEADS, DV)
    scale = lax.rsqrt(lax.optimization_barrier(jnp.mean(retained * retained, axis=-1, keepdims=True)) + HEAD_EPS)
    head_out = (retained * scale * head_gain).astype(jnp.bfloat16).reshape(TOKENS, HEADS * DV)
    middle = (tokens.astype(jnp.float32) + grouped_sum(head_out, out_w)).astype(jnp.bfloat16)
    chan_normed = norm_rows(middle, chan_gain)
    upward = jnp.dot(chan_normed, up_w, preferred_element_type=jnp.float32)
    hidden = jnp.square(jax.nn.relu(upward)).astype(jnp.bfloat16)
    return (middle.astype(jnp.float32) + grouped_sum(hidden, down_w)).astype(jnp.bfloat16)
```

```python
import functools

import jax
import jax.numpy as jnp
import numpy as np
from jax import lax
from jax.experimental import pallas as pl
from jax.experimental.pallas import tpu as pltpu
from jax.sharding import PartitionSpec as P


DK = 256
DV = 512
BLOCK = 128


EPS = 1e-06
HEAD_EPS = 0.05
THETA = 10000.0


def norm_rows(rows, gain):
    values = rows.astype(jnp.float32)
    scale = lax.rsqrt(jnp.mean(values * values, axis=-1, keepdims=True) + EPS)
    return (values * scale * gain).astype(jnp.bfloat16)


def rotate(field, places):
    half = field.shape[-1] // 2
    inverse = THETA ** (-jnp.arange(half, dtype=jnp.float32) / half)
    angles = places[:, None] * inverse
    cosine = jnp.cos(angles)[:, None, :]
    sine = jnp.sin(angles)[:, None, :]
    first = field[..., :half]
    second = field[..., half:]
    return jnp.concatenate(
        [first * cosine - second * sine, second * cosine + first * sine], axis=-1
    )


def retain(query, keys, values, log_rate):
    count = query.shape[0] // BLOCK
    q_blocks = query.reshape(count, BLOCK, query.shape[1])
    k_blocks = keys.reshape(count, BLOCK, keys.shape[1])
    v_blocks = values.reshape(count, BLOCK, values.shape[1])
    place = jnp.arange(BLOCK, dtype=jnp.float32)
    offset = place[:, None] - place[None, :]
    mask = jnp.where(offset >= 0, jnp.exp(log_rate * jnp.maximum(offset, 0.0)), 0.0)
    q_decay = jnp.exp(log_rate * (place + 1.0))
    k_decay = jnp.exp(log_rate * (BLOCK - 1.0 - place))
    block_decay = jnp.exp(log_rate * BLOCK)

    def advance(state, item):
        q_part, k_part, v_part = item
        scores = jnp.dot(q_part, k_part.T, preferred_element_type=jnp.float32)
        weights = (scores * mask).astype(jnp.bfloat16)
        result = jnp.dot(weights, v_part, preferred_element_type=jnp.float32)
        q_scaled = (q_part.astype(jnp.float32) * q_decay[:, None]).astype(jnp.bfloat16)
        result = result + jnp.dot(
            q_scaled, state.astype(jnp.bfloat16), preferred_element_type=jnp.float32
        )
        k_scaled = (k_part.astype(jnp.float32) * k_decay[:, None]).astype(jnp.bfloat16)
        state = state * block_decay + jnp.dot(
            k_scaled.T, v_part, preferred_element_type=jnp.float32
        )
        return (state, result)

    start = jnp.zeros((query.shape[1], values.shape[1]), jnp.float32)
    _, outputs = lax.scan(advance, start, (q_blocks, k_blocks, v_blocks))
    return outputs.reshape(count * BLOCK, values.shape[1])


def shards(tokens, mix_gain, query_w, key_w, value_w, head_gain, out_w, chan_gain, up_w, down_w):
    rows = tokens.shape[0]
    local = query_w.shape[1] // DK
    whole = lax.all_gather(tokens, "tp", axis=1, tiled=True)
    normed = norm_rows(whole, mix_gain)
    pieces = (
        lax.all_gather(query_w, "fs", axis=0, tiled=True),
        lax.all_gather(key_w, "fs", axis=0, tiled=True),
        lax.all_gather(value_w, "fs", axis=0, tiled=True),
    )
    inputs = normed
    qraw, kraw, vraw = tuple(
        (jnp.dot(inputs, piece, preferred_element_type=jnp.float32) for piece in pieces)
    )
    places = jnp.arange(rows, dtype=jnp.int32).astype(jnp.float32)
    query = rotate(qraw.reshape(rows, local, DK), places).astype(jnp.bfloat16)
    keys = (rotate(kraw.reshape(rows, local, DK), places) * DK ** (-0.5)).astype(jnp.bfloat16)
    values = vraw.reshape(rows, local, DV).astype(jnp.bfloat16)
    first_head = lax.axis_index("tp") * local
    heads = (first_head + jnp.arange(local, dtype=jnp.int32)).astype(jnp.float32)
    log_rate = jnp.log1p(-jnp.exp2(-5.0 - heads))
    retained = jax.vmap(retain, in_axes=(1, 1, 1, 0), out_axes=1)(query, keys, values, log_rate)
    gains = lax.dynamic_slice_in_dim(head_gain, first_head, local, 0)
    scale = lax.rsqrt(jnp.mean(retained * retained, axis=-1, keepdims=True) + HEAD_EPS)
    head_out = (retained * scale * gains).astype(jnp.bfloat16).reshape(rows, local * DV)
    mixer_terms = jnp.dot(
        head_out,
        lax.all_gather(out_w, "fs", axis=1, tiled=True),
        preferred_element_type=jnp.float32,
    )
    mixed = lax.psum_scatter(
        mixer_terms.astype(jnp.bfloat16), "tp", scatter_dimension=1, tiled=True
    ).astype(jnp.float32)
    middle = (tokens.astype(jnp.float32) + mixed).astype(jnp.bfloat16)
    whole_middle = lax.all_gather(middle, "tp", axis=1, tiled=True)
    chan_normed = norm_rows(whole_middle, chan_gain)
    inputs = chan_normed
    upward = jnp.dot(
        inputs, lax.all_gather(up_w, "fs", axis=0, tiled=True), preferred_element_type=jnp.float32
    )
    hidden = jnp.square(jax.nn.relu(upward)).astype(jnp.bfloat16)
    chan_terms = jnp.dot(
        hidden, lax.all_gather(down_w, "fs", axis=1, tiled=True), preferred_element_type=jnp.float32
    )
    channel = lax.psum_scatter(
        chan_terms.astype(jnp.bfloat16), "tp", scatter_dimension=1, tiled=True
    ).astype(jnp.float32)
    return (middle.astype(jnp.float32) + channel).astype(jnp.bfloat16)


MESH = pl.DeviceIdType.MESH
QK, VV, OUT, UP, DOWN = range(5)
KINDS = 5
LAG = 2


def loop(count, body):
    def step(index, carry):
        body(index)
        return carry

    lax.fori_loop(0, count, step, 0)


def aligned(start, size):
    return pl.ds(pl.multiple_of(start, size), size)


def mm(left, right):
    return jnp.dot(left, right, preferred_element_type=jnp.float32)


def fused_kernel(count, *refs):
    (
        tokens, query_w, key_w, value_w, out_w, up_w, down_w,
        mix_gain_in, chan_gain_in, head_gain_in, cosine_in, sine_in, rate_in,
        result,
        w_qk, w_v, w_out, w_up, w_down,
        raw, normed, acc, query, keys, values, scores, hidden,
        core_out, core_in, chip_out, chip_in, middle, last_out, last_in,
        mix_gain, chan_gain, head_gain, cosine, sine, rates,
        line_send, line_recv, cross_send, cross_recv, pair_send, pair_recv, local_sem,
        token_send, token_recv, token_local, table_sem,
        core_send, core_recv, chip_send, chip_recv, mid_send, mid_recv,
        end_core_send, end_core_recv, end_send, end_recv, result_sem,
    ) = refs
    bf16, f32 = jnp.bfloat16, jnp.float32
    rows, width = tokens.shape
    planes = count // 2
    total = 2 * rows
    full = 2 * width
    share = full // count
    per_half = count // 2
    dk, dv = DK, DV
    local = query_w.shape[1] // dk // 2
    place = lax.axis_index("fs")
    z, y = place // 2, place % 2
    x = lax.axis_index("rep")
    c = lax.axis_index("tp")
    partner = {"fs": 2 * z + 1 - y}
    twin = {"rep": 1 - x}
    sibling = {"tp": 1 - c}
    first_head = (2 * c + y) * local

    weights = (w_qk, w_v, w_out, w_up, w_down)
    by_rows = (True, True, False, True, False)
    half_q = query_w.shape[1] // 2
    subs = (
        ((query_w, 0, half_q), (key_w, half_q, half_q)),
        ((value_w, 0, value_w.shape[1] // 2),),
        ((out_w, 0, 0),),
        ((up_w, 0, up_w.shape[1] // 2),),
        ((down_w, 0, 0),),
    )

    def region(kind, origin, part):
        ref = weights[kind]
        if by_rows[kind]:
            size = ref.shape[0] // count // 2
            return ref.at[aligned(origin * (2 * size) + part * size, size), :]
        size = ref.shape[1] // 2
        return ref.at[origin, aligned(part * size, size), :]

    def piece_origin(plane, order):
        return 2 * plane + (y if order == 0 else 1 - y)

    def own_copy(kind, sub):
        source, offset, size = subs[kind][sub]
        ref = weights[kind]
        if by_rows[kind]:
            span = source.shape[0]
            return pltpu.make_async_copy(
                source.at[:, aligned(y * size, size)],
                ref.at[aligned(place * span, span), pl.ds(offset, size)],
                local_sem.at[kind, sub],
            )
        span = source.shape[0] // 2
        return pltpu.make_async_copy(
            source.at[aligned(y * span, span), :], ref.at[place], local_sem.at[kind, sub]
        )

    def pair_copy(kind, part, sub):
        source, offset, size = subs[kind][sub]
        ref = weights[kind]
        if by_rows[kind]:
            span = source.shape[0] // 2
            src = source.at[aligned(part * span, span), aligned((1 - y) * size, size)]
            dst = ref.at[aligned(place * (2 * span) + part * span, span), pl.ds(offset, size)]
        else:
            span = source.shape[0] // 4
            src = source.at[aligned((1 - y) * (2 * span) + part * span, span), :]
            dst = ref.at[place, aligned(part * span, span), :]
        return pltpu.make_async_remote_copy(
            src_ref=src, dst_ref=dst,
            send_sem=pair_send.at[kind, part, sub], recv_sem=pair_recv.at[kind, part, sub],
            device_id=partner, device_id_type=MESH,
        )

    def pair_wait(kind, part):
        for sub in range(len(subs[kind])):
            pair_copy(kind, part, sub).wait_recv()

    def line_copy(kind, plane, order, slot, target):
        spot = region(kind, piece_origin(plane, order), x)
        return pltpu.make_async_remote_copy(
            src_ref=spot, dst_ref=spot,
            send_sem=line_send.at[kind, plane, order, slot],
            recv_sem=line_recv.at[kind, plane, order],
            device_id={"fs": target}, device_id_type=MESH,
        )

    def cross_copy(kind, plane, order, part):
        spot = region(kind, piece_origin(plane, order), part)
        return pltpu.make_async_remote_copy(
            src_ref=spot, dst_ref=spot,
            send_sem=cross_send.at[kind, plane, order],
            recv_sem=cross_recv.at[kind, plane, order],
            device_id=twin, device_id_type=MESH,
        )

    orders = [
        sorted(range(planes), key=lambda p: (abs(p - here), (p < here) == (2 * here < planes)))[1:]
        for here in range(planes)
    ]

    def plane_at(step):
        found = jnp.int32(0)
        for here in range(planes):
            found = jnp.where(z == here, jnp.int32(orders[here][step]), found)
        return found

    far = [plane_at(step) for step in range(planes - 1)]

    def forward_way(plane):
        way = jnp.where(plane < z, 1, -1)
        ahead = z + way
        return (ahead >= 0) & (ahead < planes), place + 2 * way

    def send_own(kind, order):
        @pl.when(z < planes - 1)
        def _():
            line_copy(kind, z, order, 0, place + 2).start()

        @pl.when(z > 0)
        def _():
            line_copy(kind, z, order, 1, place - 2).start()

    def begin_local(kind):
        for sub in range(len(subs[kind])):
            own_copy(kind, sub).start()

    def begin_line(kind):
        for sub in range(len(subs[kind])):
            own_copy(kind, sub).wait()
        send_own(kind, 0)

    def begin_pair(kind, part):
        for sub in range(len(subs[kind])):
            pair_copy(kind, part, sub).start()

    def pair_line(kind):
        pair_wait(kind, x)
        send_own(kind, 1)

    def service(kind, step, order):
        plane = far[step]
        line_copy(kind, plane, order, 0, place).wait_recv()
        going, target = forward_way(plane)

        @pl.when(going)
        def _():
            line_copy(kind, plane, order, 0, target).start()

        cross_copy(kind, plane, order, x).start()

    def arrived(kind, step, order):
        cross_copy(kind, far[step], order, 1 - x).wait_recv()

    def token_copy(index):
        own = raw.at[y, c]
        if index == 0:
            spot, target = own, sibling
        elif index == 1:
            spot, target = own, partner
        else:
            spot, target = raw.at[1 - y, c], sibling
        return pltpu.make_async_remote_copy(
            src_ref=spot, dst_ref=spot, send_sem=token_send.at[index],
            recv_sem=token_recv.at[index], device_id=target, device_id_type=MESH,
        )

    tables = (
        (mix_gain_in, mix_gain), (chan_gain_in, chan_gain), (head_gain_in, head_gain),
        (cosine_in, cosine), (sine_in, sine), (rate_in, rates),
    )

    def table_copy(index):
        return pltpu.make_async_copy(tables[index][0], tables[index][1], table_sem.at[index])

    own_tokens = pltpu.make_async_copy(tokens, raw.at[y, c], token_local)

    def norm_first():
        size = 64

        def tile(index):
            for p in range(2):
                span = aligned(index * size, size)
                left = raw[p, 0, span, :].astype(f32)
                right = raw[p, 1, span, :].astype(f32)
                mean = (
                    jnp.sum(left * left, axis=-1, keepdims=True)
                    + jnp.sum(right * right, axis=-1, keepdims=True)
                ) / full
                scale = lax.rsqrt(mean + EPS)
                put = aligned(p * rows + index * size, size)
                normed[put, :width] = (left * scale * mix_gain[:, :width]).astype(bf16)
                normed[put, width:] = (right * scale * mix_gain[:, width:]).astype(bf16)

        loop(rows // size, tile)

    def accumulate(kind, origin, first):
        ref = weights[kind]
        base = 0 if kind == QK else w_qk.shape[1]
        high, wide = min(256, total), min(512, ref.shape[1])
        across = ref.shape[1] // wide

        def tile(index):
            span = aligned(index // across * high, high)
            right = ref[aligned(origin * share, share), aligned(index % across * wide, wide)]
            term = mm(normed[span, aligned(origin * share, share)], right)
            put = aligned(base + index % across * wide, wide)
            if first:
                acc[span, put] = term
            else:
                acc[span, put] += term

        loop(total // high * across, tile)

    def turn():
        size = 128
        half = dk // 2

        def tile(index):
            for p in range(2):
                inner = aligned(index * size, size)
                span = aligned(p * rows + index * size, size)
                cos, sin = cosine[inner, :], sine[inner, :]
                for head in range(local):
                    for base, ref, scale in ((0, query, None), (half_q, keys, dk ** (-0.5))):
                        at = head * dk
                        one = acc[span, base + at : base + at + half]
                        two = acc[span, base + at + half : base + at + dk]
                        low, top = one * cos - two * sin, two * cos + one * sin
                        if scale is not None:
                            low, top = low * scale, top * scale
                        ref[span, at : at + half] = low.astype(bf16)
                        ref[span, at + half : at + dk] = top.astype(bf16)

        loop(rows // size, tile)

    strip = min(256, rows)

    def score(p, head):
        rate = rates[pl.ds(first_head + head, 1), 0:1]
        lanes = slice(head * dk, (head + 1) * dk)
        for block in range(rows // strip):
            seen = (block + 1) * strip
            q_part = query[p * rows + block * strip : p * rows + seen, lanes]
            k_part = keys[p * rows : p * rows + seen, lanes]
            product = lax.dot_general(
                q_part, k_part, (((1,), (1,)), ((), ())), preferred_element_type=f32
            )
            offset = (
                lax.broadcasted_iota(jnp.int32, (strip, seen), 0)
                - lax.broadcasted_iota(jnp.int32, (strip, seen), 1)
                + block * strip
            )
            decay = jnp.exp(rate * jnp.maximum(offset, 0).astype(f32))
            decay = jnp.where(offset >= 0, decay, 0.0)
            scores[p * local + head, block * strip : seen, :seen] = (product * decay).astype(bf16)

    def take_values():
        size = 128

        def tile(index):
            span = aligned(index * size, size)
            values[span, :] = acc[span, w_qk.shape[1] :].astype(bf16)

        loop(total // size, tile)

    def retain_head(p, head):
        gain = head_gain[pl.ds(first_head + head, 1), :]
        lanes = slice(head * dv, (head + 1) * dv)
        for block in range(rows // strip):
            seen = (block + 1) * strip
            got = mm(
                scores[p * local + head, block * strip : seen, :seen],
                values[p * rows : p * rows + seen, lanes],
            )
            mean = jnp.sum(got * got, axis=-1, keepdims=True) / dv
            scale = lax.rsqrt(mean + HEAD_EPS)
            hidden[p * rows + block * strip : p * rows + seen, lanes] = (
                got * scale * gain
            ).astype(bf16)

    high = min(256, total)

    def mine(origin):
        return origin // per_half == c

    def lane(origin):
        return aligned(origin % per_half * share, share)

    def core_copy(plane):
        first = 2 * plane % per_half
        return pltpu.make_async_remote_copy(
            src_ref=core_out.at[pl.ds(first, 2)], dst_ref=core_in.at[pl.ds(first, 2)],
            send_sem=core_send.at[first // 2], recv_sem=core_recv.at[first // 2],
            device_id=sibling, device_id_type=MESH,
        )

    def chip_copy(plane):
        first = 2 * plane % per_half
        return pltpu.make_async_remote_copy(
            src_ref=chip_out.at[pl.ds(first, 2)], dst_ref=chip_in.at[pl.ds(first, 2)],
            send_sem=chip_send.at[first // 2], recv_sem=chip_recv.at[first // 2],
            device_id=partner, device_id_type=MESH,
        )

    def middle_copy(plane):
        spot = middle.at[pl.ds(2 * plane, 2)]
        return pltpu.make_async_remote_copy(
            src_ref=spot, dst_ref=spot, send_sem=mid_send.at[plane], recv_sem=mid_recv.at[plane],
            device_id=sibling, device_id_type=MESH,
        )

    def product(ref, origin, keep):
        def tile(index):
            span = aligned(index * high, high)
            term = mm(hidden[span, :], ref[origin])
            if keep:
                acc[span, lane(origin)] = term
            else:
                core_out[origin % per_half, span, :] = term.astype(bf16)

        loop(total // high, tile)

    def mix_partial(plane):
        @pl.when(mine(2 * plane))
        def _():
            for pick in range(2):
                product(w_out, 2 * plane + pick, True)

        @pl.when(jnp.logical_not(mine(2 * plane)))
        def _():
            for pick in range(2):
                product(w_out, 2 * plane + pick, False)
            core_copy(plane).start()

    def mix_combine(plane):
        @pl.when(mine(2 * plane))
        def _():
            core_copy(plane).wait_recv()
            for pick in range(2):
                origin = 2 * plane + pick

                def tile(index, origin=origin):
                    span = aligned(index * high, high)
                    chip_out[origin % per_half, span, :] = (
                        acc[span, lane(origin)] + core_in[origin % per_half, span, :].astype(f32)
                    ).astype(bf16)

                loop(total // high, tile)
            chip_copy(plane).start()

    def mix_finish(plane):
        @pl.when(mine(2 * plane))
        def _():
            chip_copy(plane).wait_recv()
            for pick in range(2):
                origin = 2 * plane + pick
                for p in range(2):

                    def tile(index, origin=origin, p=p):
                        inner = aligned(index * high, high)
                        span = aligned(p * rows + index * high, high)
                        at = origin % per_half
                        mixed = chip_out[at, span, :].astype(f32) + chip_in[at, span, :].astype(f32)
                        middle[origin, span, :] = (
                            raw[p, c, inner, lane(origin)].astype(f32) + mixed
                        ).astype(bf16)

                    loop(rows // high, tile)
            middle_copy(plane).start()

    def mix_settle(plane):
        @pl.when(jnp.logical_not(mine(2 * plane)))
        def _():
            middle_copy(plane).wait_recv()

    def norm_second():
        size = 64

        def tile(index):
            span = aligned(index * size, size)
            strips = [middle[origin, span, :].astype(f32) for origin in range(count)]
            mean = sum(jnp.sum(s * s, axis=-1, keepdims=True) for s in strips) / full
            scale = lax.rsqrt(mean + EPS)
            for origin in range(count):
                lanes = slice(origin * share, (origin + 1) * share)
                normed[span, lanes] = (strips[origin] * scale * chan_gain[:, lanes]).astype(bf16)

        loop(total // size, tile)

    def upward():
        wide = min(512, w_up.shape[1])
        across = w_up.shape[1] // wide

        def tile(index):
            span = aligned(index // across * high, high)
            lanes = aligned(index % across * wide, wide)
            got = jnp.maximum(mm(normed[span, :], w_up[:, lanes]), 0.0)
            hidden[span, lanes] = (got * got).astype(bf16)

        loop(total // high * across, tile)

    def end_core_copy(origin):
        at = origin % per_half
        return pltpu.make_async_remote_copy(
            src_ref=core_out.at[at], dst_ref=core_in.at[at],
            send_sem=end_core_send.at[at], recv_sem=end_core_recv.at[at],
            device_id=sibling, device_id_type=MESH,
        )

    def end_copy(origin):
        at = origin % per_half
        return pltpu.make_async_remote_copy(
            src_ref=last_out.at[at], dst_ref=last_in.at[at],
            send_sem=end_send.at[at], recv_sem=end_recv.at[at],
            device_id=partner, device_id_type=MESH,
        )

    def result_copy(origin):
        at = origin % per_half
        return pltpu.make_async_copy(
            values.at[aligned(at // 2 * rows, rows), aligned(at % 2 * share, share)],
            result.at[:, lane(origin)],
            result_sem.at[at],
        )

    def end_partial(origin):
        @pl.when(mine(origin))
        def _():
            product(w_down, origin, True)

        @pl.when(jnp.logical_not(mine(origin)))
        def _():
            product(w_down, origin, False)
            end_core_copy(origin).start()

    def end_combine(origin):
        @pl.when(mine(origin))
        def _():
            end_core_copy(origin).wait_recv()
            at = origin % per_half

            def tile(index):
                span = aligned((1 - y) * rows + index * high, high)
                last_out[at, aligned(index * high, high), :] = (
                    acc[span, lane(origin)] + core_in[at, span, :].astype(f32)
                ).astype(bf16)

            loop(rows // high, tile)
            end_copy(origin).start()

    def end_finish(origin):
        @pl.when(mine(origin))
        def _():
            end_copy(origin).wait_recv()
            at = origin % per_half

            def tile(index):
                inner = aligned(index * high, high)
                span = aligned(y * rows + index * high, high)
                added = acc[span, lane(origin)] + core_in[at, span, :].astype(f32)
                added = added + last_in[at, inner, :].astype(f32)
                put = aligned(at // 2 * rows + index * high, high)
                values[put, aligned(at % 2 * share, share)] = (
                    middle[origin, span, :].astype(f32) + added
                ).astype(bf16)

            loop(rows // high, tile)
            result_copy(origin).start()

    begin_local(QK)
    own_tokens.start()
    for index in range(len(tables)):
        table_copy(index).start()
    barrier = pltpu.get_barrier_semaphore()
    for other in (partner, twin, sibling):
        pl.semaphore_signal(barrier, inc=1, device_id=other, device_id_type=MESH)

    @pl.when(z < planes - 1)
    def _():
        pl.semaphore_signal(barrier, inc=1, device_id={"fs": place + 2}, device_id_type=MESH)

    @pl.when(z > 0)
    def _():
        pl.semaphore_signal(barrier, inc=1, device_id={"fs": place - 2}, device_id_type=MESH)

    pl.semaphore_wait(
        barrier, 3 + jnp.where(z < planes - 1, 1, 0) + jnp.where(z > 0, 1, 0)
    )
    begin_pair(QK, x)
    begin_line(QK)
    own_tokens.wait()
    token_copy(0).start()
    token_copy(1).start()
    begin_pair(QK, 1 - x)
    begin_local(VV)
    begin_pair(VV, x)
    begin_pair(VV, 1 - x)
    pair_line(QK)

    def own_pair(kind, task):
        def first():
            task(piece_origin(z, 0))

        def second():
            pair_wait(kind, 1 - x)
            task(piece_origin(z, 1))

        return first, second

    def chunk(kind, step, order, task):
        def run():
            arrived(kind, step, order)
            task(piece_origin(far[step], order))

        return run

    slots = planes - 1
    span = 2 * slots
    plan = {}

    def at(slot, *tasks):
        plan.setdefault(slot, []).extend(tasks)

    def start_tokens():
        token_copy(1).wait_recv()
        token_copy(2).start()

    def first_norm():
        for index in range(len(tables)):
            table_copy(index).wait()
        token_copy(0).wait_recv()
        token_copy(2).wait_recv()
        norm_first()

    last = KINDS * span - 1
    at(4, start_tokens)
    at(5, first_norm)
    own_qk = own_pair(QK, lambda o: accumulate(QK, o, False))
    at(6, lambda: accumulate(QK, piece_origin(z, 0), True), own_qk[1])
    own_v = own_pair(VV, lambda o: accumulate(VV, o, False))
    at(10, lambda: accumulate(VV, piece_origin(z, 0), True), own_v[1])
    for number in range(span):
        step, order = number // 2, number % 2
        at(
            max(number + LAG, 7 + number // 2),
            chunk(QK, step, order, lambda o: accumulate(QK, o, False)),
        )
        at(
            max(number + span + LAG, 10 + number // 2),
            chunk(VV, step, order, lambda o: accumulate(VV, o, False)),
        )
    at(10, turn)
    for p in range(2):
        for head in range(local):
            at(11 + p, functools.partial(score, p, head))
    at(2 * span + LAG - 1, take_values)
    for p in range(2):
        for head in range(local):
            at(2 * span + LAG - 1 + p, functools.partial(retain_head, p, head))
    base = 2 * span + LAG

    def ready(kind, step):
        def run():
            if step < 0:
                pair_wait(kind, 1 - x)
            else:
                for order in range(2):
                    arrived(kind, step, order)

        return run

    def plane_of(step):
        return z if step < 0 else far[step]

    at(base, ready(OUT, -1), lambda: mix_partial(z))
    at(base + 1, lambda: mix_combine(z))
    for step in range(slots):
        when = max(2 * span + 2 * step + 1 + LAG, base + 1)
        at(when, ready(OUT, step), functools.partial(mix_partial, far[step]))
        at(when + 1, functools.partial(mix_combine, far[step]))
    for number in range(planes):
        plane = plane_of(number - 1)
        at(base + 4 + 2 * number, functools.partial(mix_finish, plane))
        at(base + 5 + 2 * number, functools.partial(mix_settle, plane))
    finish = base + 5 + 2 * (planes - 1)

    def third_norm():
        for step in range(-1, slots):
            plane = plane_of(step)

            @pl.when(jnp.logical_not(mine(2 * plane)))
            def _(plane=plane):
                core_copy(plane).wait_send()

        norm_second()

    at(finish, third_norm)

    def up_all():
        for step in range(-1, slots):
            ready(UP, step)()
        upward()

    at(finish + 1, up_all)
    chunks = [piece_origin(z, 0), piece_origin(z, 1)]
    for step in range(slots):
        chunks += [piece_origin(far[step], order) for order in range(2)]

    def down_ready(number):
        def run():
            if number == 1:
                pair_wait(DOWN, 1 - x)
            elif number > 1:
                arrived(DOWN, (number - 2) // 2, number % 2)

        return run

    early = min(count - 2, span + 2 - LAG)
    for number in range(count):
        when = finish + 2 + number // 3
        arrive = 4 * span + (number - 2) + LAG
        when = min(max(when, arrive), last + 1) if number < count - 2 else last + 1
        at(when, down_ready(number), functools.partial(end_partial, chunks[number]))
        at(when if number >= count - 3 else when, functools.partial(end_combine, chunks[number]))
    for number in range(count):
        at(last + 2, functools.partial(end_finish, chunks[number]))

    def run_plan(slot):
        for task in plan.pop(slot, ()):
            task()

    for kind in range(KINDS):
        for step in range(slots):
            for order in range(2):
                if step == slots - 1 and order == 1 and kind + 1 < KINDS:
                    begin_line(kind + 1)
                service(kind, step, order)
                if step == slots - 1 and order == 1 and kind + 1 < KINDS:
                    pair_line(kind + 1)
                if step == 0 and order == 0 and kind + 2 < KINDS:
                    begin_local(kind + 2)
                    begin_pair(kind + 2, x)
                    begin_pair(kind + 2, 1 - x)
                run_plan(kind * span + 2 * step + order)
    for slot in sorted(plan):
        run_plan(slot)
    for kind in range(KINDS):
        for sub in range(len(subs[kind])):
            for part in range(2):
                pair_copy(kind, part, sub).wait_send()
        for order in range(2):

            @pl.when(z < planes - 1)
            def _(kind=kind, order=order):
                line_copy(kind, z, order, 0, place + 2).wait_send()

            @pl.when(z > 0)
            def _(kind=kind, order=order):
                line_copy(kind, z, order, 1, place - 2).wait_send()

        for step in range(slots):
            going, target = forward_way(far[step])
            for order in range(2):

                @pl.when(going)
                def _(kind=kind, order=order, step=step, target=target):
                    line_copy(kind, far[step], order, 0, target).wait_send()

                cross_copy(kind, far[step], order, x).wait_send()
    for index in range(3):
        token_copy(index).wait_send()
    for plane in range(planes):

        @pl.when(mine(2 * plane))
        def _(plane=plane):
            chip_copy(plane).wait_send()
            middle_copy(plane).wait_send()

    for origin in range(count):

        @pl.when(mine(origin))
        def _(origin=origin):
            end_copy(origin).wait_send()
            result_copy(origin).wait()

        @pl.when(jnp.logical_not(mine(origin)))
        def _(origin=origin):
            end_core_copy(origin).wait_send()


def fused_layer(
    count, tokens, mix_gain, query_w, key_w, value_w, head_gain, out_w, chan_gain, up_w, down_w
):
    rows, width = tokens.shape
    total, full = 2 * rows, 2 * width
    planes = count // 2
    per_half = count // 2
    share = full // count
    q_cols = query_w.shape[1] // 2
    v_cols = value_w.shape[1] // 2
    ff_cols = up_w.shape[1] // 2
    local = q_cols // DK
    half = DK // 2
    spots = np.arange(rows, dtype=np.float32)
    inverse = np.float32(THETA) ** (-np.arange(half, dtype=np.float32) / np.float32(half))
    angles = spots[:, None] * inverse.astype(np.float32)
    heads = np.arange(head_gain.shape[0], dtype=np.float32)
    rate = np.log1p(-np.exp2(np.float32(-5.0) - heads)).astype(np.float32)
    rate = np.repeat(rate[:, None], 128, axis=1)
    bf16, f32 = jnp.bfloat16, jnp.float32
    dma = pltpu.SemaphoreType.DMA
    vmem = pltpu.VMEM
    scratch = [
        vmem((full, 2 * q_cols), bf16), vmem((full, v_cols), bf16),
        vmem((count, v_cols, share), bf16), vmem((full, ff_cols), bf16),
        vmem((count, ff_cols, share), bf16),
        vmem((2, 2, rows, width), bf16), vmem((total, full), bf16),
        vmem((total, 2 * q_cols + v_cols), f32),
        vmem((total, q_cols), bf16), vmem((total, q_cols), bf16), vmem((total, v_cols), bf16),
        vmem((2 * local, rows, rows), bf16), vmem((total, v_cols), bf16),
        vmem((per_half, total, share), bf16), vmem((per_half, total, share), bf16),
        vmem((per_half, total, share), bf16), vmem((per_half, total, share), bf16),
        vmem((count, total, share), bf16),
        vmem((per_half, rows, share), bf16), vmem((per_half, rows, share), bf16),
        vmem((1, full), f32), vmem((1, full), f32), vmem(head_gain.shape, f32),
        vmem((rows, half), f32), vmem((rows, half), f32), vmem(rate.shape, f32),
        dma((KINDS, planes, 2, 2)), dma((KINDS, planes, 2)),
        dma((KINDS, planes, 2)), dma((KINDS, planes, 2)),
        dma((KINDS, 2, 2)), dma((KINDS, 2, 2)), dma((KINDS, 2)),
        dma((3,)), dma((3,)), dma, dma((6,)),
        dma((planes // 2,)), dma((planes // 2,)), dma((planes // 2,)), dma((planes // 2,)),
        dma((planes,)), dma((planes,)),
        dma((per_half,)), dma((per_half,)), dma((per_half,)), dma((per_half,)), dma((per_half,)),
    ]
    return pl.pallas_call(
        functools.partial(fused_kernel, count),
        out_shape=jax.ShapeDtypeStruct((rows, width), bf16),
        in_specs=[pl.BlockSpec(memory_space=pl.ANY)] * 13,
        out_specs=pl.BlockSpec(memory_space=pl.ANY),
        scratch_shapes=scratch,
        compiler_params=pltpu.CompilerParams(
            collective_id=0, has_side_effects=True, vmem_limit_bytes=67_043_328
        ),
        name="fused_layer",
    )(
        tokens, query_w, key_w, value_w, out_w, up_w, down_w,
        mix_gain.reshape(1, full), chan_gain.reshape(1, full), head_gain,
        jnp.asarray(np.cos(angles)), jnp.asarray(np.sin(angles)), jnp.asarray(rate),
    )


def solution(mesh):
    placed = (
        P(("rep", "fs"), "tp"),
        P(),
        P("fs", "tp"),
        P("fs", "tp"),
        P("fs", "tp"),
        P(),
        P("tp", "fs"),
        P(),
        P("fs", "tp"),
        P("tp", "fs"),
    )
    parts, tps, count = mesh.shape["rep"], mesh.shape["tp"], mesh.shape["fs"]

    def body(*blocks):
        heads = blocks[2].shape[1] // DK
        if parts == 2 and tps == 2 and count % 4 == 0 and heads % 2 == 0:
            return fused_layer(count, *blocks)
        return shards(*blocks)

    return jax.shard_map(
        body, mesh=mesh, in_specs=placed, out_specs=P(("rep", "fs"), "tp"), check_vma=False
    )
```

```python
import functools

import jax
import jax.numpy as jnp
import numpy as np
from jax import lax
from jax.experimental import pallas as pl
from jax.experimental.pallas import tpu as pltpu
from jax.sharding import PartitionSpec as P


DK = 256
DV = 512
BLOCK = 128


EPS = 1e-06
HEAD_EPS = 0.05
THETA = 10000.0


def norm_rows(rows, gain):
    values = rows.astype(jnp.float32)
    scale = lax.rsqrt(jnp.mean(values * values, axis=-1, keepdims=True) + EPS)
    return (values * scale * gain).astype(jnp.bfloat16)


def rotate(field, places):
    half = field.shape[-1] // 2
    inverse = THETA ** (-jnp.arange(half, dtype=jnp.float32) / half)
    angles = places[:, None] * inverse
    cosine = jnp.cos(angles)[:, None, :]
    sine = jnp.sin(angles)[:, None, :]
    first = field[..., :half]
    second = field[..., half:]
    return jnp.concatenate(
        [first * cosine - second * sine, second * cosine + first * sine], axis=-1
    )


def retain(query, keys, values, log_rate):
    count = query.shape[0] // BLOCK
    q_blocks = query.reshape(count, BLOCK, query.shape[1])
    k_blocks = keys.reshape(count, BLOCK, keys.shape[1])
    v_blocks = values.reshape(count, BLOCK, values.shape[1])
    place = jnp.arange(BLOCK, dtype=jnp.float32)
    offset = place[:, None] - place[None, :]
    mask = jnp.where(offset >= 0, jnp.exp(log_rate * jnp.maximum(offset, 0.0)), 0.0)
    q_decay = jnp.exp(log_rate * (place + 1.0))
    k_decay = jnp.exp(log_rate * (BLOCK - 1.0 - place))
    block_decay = jnp.exp(log_rate * BLOCK)

    def advance(state, item):
        q_part, k_part, v_part = item
        scores = jnp.dot(q_part, k_part.T, preferred_element_type=jnp.float32)
        weights = (scores * mask).astype(jnp.bfloat16)
        result = jnp.dot(weights, v_part, preferred_element_type=jnp.float32)
        q_scaled = (q_part.astype(jnp.float32) * q_decay[:, None]).astype(jnp.bfloat16)
        result = result + jnp.dot(
            q_scaled, state.astype(jnp.bfloat16), preferred_element_type=jnp.float32
        )
        k_scaled = (k_part.astype(jnp.float32) * k_decay[:, None]).astype(jnp.bfloat16)
        state = state * block_decay + jnp.dot(
            k_scaled.T, v_part, preferred_element_type=jnp.float32
        )
        return (state, result)

    start = jnp.zeros((query.shape[1], values.shape[1]), jnp.float32)
    _, outputs = lax.scan(advance, start, (q_blocks, k_blocks, v_blocks))
    return outputs.reshape(count * BLOCK, values.shape[1])


def shards(tokens, mix_gain, query_w, key_w, value_w, head_gain, out_w, chan_gain, up_w, down_w):
    rows = tokens.shape[0]
    local = query_w.shape[1] // DK
    whole = lax.all_gather(tokens, "tp", axis=1, tiled=True)
    normed = norm_rows(whole, mix_gain)
    pieces = (
        lax.all_gather(query_w, "fs", axis=0, tiled=True),
        lax.all_gather(key_w, "fs", axis=0, tiled=True),
        lax.all_gather(value_w, "fs", axis=0, tiled=True),
    )
    inputs = normed
    qraw, kraw, vraw = tuple(
        (jnp.dot(inputs, piece, preferred_element_type=jnp.float32) for piece in pieces)
    )
    places = jnp.arange(rows, dtype=jnp.int32).astype(jnp.float32)
    query = rotate(qraw.reshape(rows, local, DK), places).astype(jnp.bfloat16)
    keys = (rotate(kraw.reshape(rows, local, DK), places) * DK ** (-0.5)).astype(jnp.bfloat16)
    values = vraw.reshape(rows, local, DV).astype(jnp.bfloat16)
    first_head = lax.axis_index("tp") * local
    heads = (first_head + jnp.arange(local, dtype=jnp.int32)).astype(jnp.float32)
    log_rate = jnp.log1p(-jnp.exp2(-5.0 - heads))
    retained = jax.vmap(retain, in_axes=(1, 1, 1, 0), out_axes=1)(query, keys, values, log_rate)
    gains = lax.dynamic_slice_in_dim(head_gain, first_head, local, 0)
    scale = lax.rsqrt(jnp.mean(retained * retained, axis=-1, keepdims=True) + HEAD_EPS)
    head_out = (retained * scale * gains).astype(jnp.bfloat16).reshape(rows, local * DV)
    mixer_terms = jnp.dot(
        head_out,
        lax.all_gather(out_w, "fs", axis=1, tiled=True),
        preferred_element_type=jnp.float32,
    )
    mixed = lax.psum_scatter(
        mixer_terms.astype(jnp.bfloat16), "tp", scatter_dimension=1, tiled=True
    ).astype(jnp.float32)
    middle = (tokens.astype(jnp.float32) + mixed).astype(jnp.bfloat16)
    whole_middle = lax.all_gather(middle, "tp", axis=1, tiled=True)
    chan_normed = norm_rows(whole_middle, chan_gain)
    inputs = chan_normed
    upward = jnp.dot(
        inputs, lax.all_gather(up_w, "fs", axis=0, tiled=True), preferred_element_type=jnp.float32
    )
    hidden = jnp.square(jax.nn.relu(upward)).astype(jnp.bfloat16)
    chan_terms = jnp.dot(
        hidden, lax.all_gather(down_w, "fs", axis=1, tiled=True), preferred_element_type=jnp.float32
    )
    channel = lax.psum_scatter(
        chan_terms.astype(jnp.bfloat16), "tp", scatter_dimension=1, tiled=True
    ).astype(jnp.float32)
    return (middle.astype(jnp.float32) + channel).astype(jnp.bfloat16)


MESH = pl.DeviceIdType.MESH
QK, VV, OUT, UP, DOWN = range(5)
KINDS = 5
LAG = 2


def loop(count, body):
    def step(index, carry):
        body(index)
        return carry

    lax.fori_loop(0, count, step, 0)


def aligned(start, size):
    return pl.ds(pl.multiple_of(start, size), size)


def mm(left, right):
    return jnp.dot(left, right, preferred_element_type=jnp.float32)


def fused_kernel(count, *refs):
    (
        tokens, query_w, key_w, value_w, out_w, up_w, down_w,
        mix_gain_in, chan_gain_in, head_gain_in, cosine_in, sine_in, rate_in,
        result,
        w_qk, w_v, w_out, w_up, w_down,
        raw, normed, acc, query, keys, values, scores, hidden,
        core_out, core_in, chip_out, chip_in, middle, last_out, last_in,
        mix_gain, chan_gain, head_gain, cosine, sine, rates,
        line_send, line_recv, whole_send, whole_recv, cross_send, cross_recv, pair_send, pair_recv, local_sem,
        token_send, token_recv, token_local, table_sem,
        core_send, core_recv, chip_send, chip_recv, mid_send, mid_recv,
        end_core_send, end_core_recv, end_send, end_recv, result_sem,
    ) = refs
    bf16, f32 = jnp.bfloat16, jnp.float32
    rows, width = tokens.shape
    planes = count // 2
    total = 2 * rows
    full = 2 * width
    share = full // count
    per_half = count // 2
    dk, dv = DK, DV
    local = query_w.shape[1] // dk // 2
    place = lax.axis_index("fs")
    z, y = place // 2, place % 2
    x = lax.axis_index("rep")
    c = lax.axis_index("tp")
    partner = {"fs": 2 * z + 1 - y}
    twin = {"rep": 1 - x}
    sibling = {"tp": 1 - c}
    first_head = (2 * c + y) * local

    weights = (w_qk, w_v, w_out, w_up, w_down)
    by_rows = (True, True, False, True, False)
    half_q = query_w.shape[1] // 2
    subs = (
        ((query_w, 0, half_q), (key_w, half_q, half_q)),
        ((value_w, 0, value_w.shape[1] // 2),),
        ((out_w, 0, 0),),
        ((up_w, 0, up_w.shape[1] // 2),),
        ((down_w, 0, 0),),
    )

    def region(kind, origin, part):
        ref = weights[kind]
        if by_rows[kind]:
            size = ref.shape[0] // count // 2
            return ref.at[aligned(origin * (2 * size) + part * size, size), :]
        size = ref.shape[1] // 2
        return ref.at[origin, aligned(part * size, size), :]

    def piece_origin(plane, order):
        return 2 * plane + (y if order == 0 else 1 - y)

    def own_copy(kind, sub):
        source, offset, size = subs[kind][sub]
        ref = weights[kind]
        if by_rows[kind]:
            span = source.shape[0]
            return pltpu.make_async_copy(
                source.at[:, aligned(y * size, size)],
                ref.at[aligned(place * span, span), pl.ds(offset, size)],
                local_sem.at[kind, sub],
            )
        span = source.shape[0] // 2
        return pltpu.make_async_copy(
            source.at[aligned(y * span, span), :], ref.at[place], local_sem.at[kind, sub]
        )

    def pair_copy(kind, part, sub):
        source, offset, size = subs[kind][sub]
        ref = weights[kind]
        if by_rows[kind]:
            span = source.shape[0] // 2
            src = source.at[aligned(part * span, span), aligned((1 - y) * size, size)]
            dst = ref.at[aligned(place * (2 * span) + part * span, span), pl.ds(offset, size)]
        else:
            span = source.shape[0] // 4
            src = source.at[aligned((1 - y) * (2 * span) + part * span, span), :]
            dst = ref.at[place, aligned(part * span, span), :]
        return pltpu.make_async_remote_copy(
            src_ref=src, dst_ref=dst,
            send_sem=pair_send.at[kind, part, sub], recv_sem=pair_recv.at[kind, part, sub],
            device_id=partner, device_id_type=MESH,
        )

    def pair_wait(kind, part):
        for sub in range(len(subs[kind])):
            pair_copy(kind, part, sub).wait_recv()

    def line_copy(kind, plane, order, slot, target):
        spot = region(kind, piece_origin(plane, order), x)
        return pltpu.make_async_remote_copy(
            src_ref=spot, dst_ref=spot,
            send_sem=line_send.at[kind, plane, order, slot],
            recv_sem=line_recv.at[kind, plane, order],
            device_id={"fs": target}, device_id_type=MESH,
        )

    def cross_copy(kind, plane, order, part):
        spot = region(kind, piece_origin(plane, order), part)
        return pltpu.make_async_remote_copy(
            src_ref=spot, dst_ref=spot,
            send_sem=cross_send.at[kind, plane, order],
            recv_sem=cross_recv.at[kind, plane, order],
            device_id=twin, device_id_type=MESH,
        )

    def whole(kind, plane, order):
        if (kind, order) != (DOWN, 1):
            return None
        return (plane == 0) | (plane == planes - 1)

    def whole_copy(plane, slot, target):
        spot = region(DOWN, piece_origin(plane, 1), 1 - x)
        return pltpu.make_async_remote_copy(
            src_ref=spot, dst_ref=spot,
            send_sem=whole_send.at[plane, slot], recv_sem=whole_recv.at[plane],
            device_id={"fs": target}, device_id_type=MESH,
        )

    orders = [
        sorted(range(planes), key=lambda p: (abs(p - here), (p < here) == (2 * here < planes)))[1:]
        for here in range(planes)
    ]

    def plane_at(step):
        found = jnp.int32(0)
        for here in range(planes):
            found = jnp.where(z == here, jnp.int32(orders[here][step]), found)
        return found

    far = [plane_at(step) for step in range(planes - 1)]

    def forward_way(plane):
        way = jnp.where(plane < z, 1, -1)
        ahead = z + way
        return (ahead >= 0) & (ahead < planes), place + 2 * way

    def send_own(kind, order):
        @pl.when(z < planes - 1)
        def _():
            line_copy(kind, z, order, 0, place + 2).start()

        @pl.when(z > 0)
        def _():
            line_copy(kind, z, order, 1, place - 2).start()

    def begin_local(kind):
        for sub in range(len(subs[kind])):
            own_copy(kind, sub).start()

    def begin_line(kind):
        for sub in range(len(subs[kind])):
            own_copy(kind, sub).wait()
        send_own(kind, 0)

    def begin_pair(kind, part):
        for sub in range(len(subs[kind])):
            pair_copy(kind, part, sub).start()

    def pair_line(kind):
        pair_wait(kind, x)
        send_own(kind, 1)
        if whole(kind, z, 1) is not None:
            pair_wait(kind, 1 - x)

            @pl.when(z == 0)
            def _():
                whole_copy(z, 0, place + 2).start()

            @pl.when(z == planes - 1)
            def _():
                whole_copy(z, 1, place - 2).start()

    def service(kind, step, order):
        plane = far[step]
        line_copy(kind, plane, order, 0, place).wait_recv()
        going, target = forward_way(plane)

        @pl.when(going)
        def _():
            line_copy(kind, plane, order, 0, target).start()

        entire = whole(kind, plane, order)
        if entire is None:
            cross_copy(kind, plane, order, x).start()
            return

        @pl.when(jnp.logical_not(entire))
        def _():
            cross_copy(kind, plane, order, x).start()

        @pl.when(entire & going)
        def _():
            whole_copy(plane, 0, place).wait_recv()
            whole_copy(plane, 0, target).start()

    def arrived(kind, step, order):
        plane = far[step]
        entire = whole(kind, plane, order)
        if entire is None:
            cross_copy(kind, plane, order, 1 - x).wait_recv()
            return

        @pl.when(jnp.logical_not(entire))
        def _():
            cross_copy(kind, plane, order, 1 - x).wait_recv()

        @pl.when(entire & jnp.logical_not(forward_way(plane)[0]))
        def _():
            whole_copy(plane, 0, place).wait_recv()

    def token_copy(index):
        own = raw.at[y, c]
        if index == 0:
            spot, target = own, sibling
        elif index == 1:
            spot, target = own, partner
        else:
            spot, target = raw.at[1 - y, c], sibling
        return pltpu.make_async_remote_copy(
            src_ref=spot, dst_ref=spot, send_sem=token_send.at[index],
            recv_sem=token_recv.at[index], device_id=target, device_id_type=MESH,
        )

    tables = (
        (mix_gain_in, mix_gain), (chan_gain_in, chan_gain), (head_gain_in, head_gain),
        (cosine_in, cosine), (sine_in, sine), (rate_in, rates),
    )

    def table_copy(index):
        return pltpu.make_async_copy(tables[index][0], tables[index][1], table_sem.at[index])

    own_tokens = pltpu.make_async_copy(tokens, raw.at[y, c], token_local)

    def norm_first():
        size = 64

        def tile(index):
            for p in range(2):
                span = aligned(index * size, size)
                left = raw[p, 0, span, :].astype(f32)
                right = raw[p, 1, span, :].astype(f32)
                mean = (
                    jnp.sum(left * left, axis=-1, keepdims=True)
                    + jnp.sum(right * right, axis=-1, keepdims=True)
                ) / full
                scale = lax.rsqrt(mean + EPS)
                put = aligned(p * rows + index * size, size)
                normed[put, :width] = (left * scale * mix_gain[:, :width]).astype(bf16)
                normed[put, width:] = (right * scale * mix_gain[:, width:]).astype(bf16)

        loop(rows // size, tile)

    def accumulate(kind, origin, first):
        ref = weights[kind]
        base = 0 if kind == QK else w_qk.shape[1]
        high, wide = min(256, total), min(512, ref.shape[1])
        across = ref.shape[1] // wide

        def tile(index):
            span = aligned(index // across * high, high)
            right = ref[aligned(origin * share, share), aligned(index % across * wide, wide)]
            term = mm(normed[span, aligned(origin * share, share)], right)
            put = aligned(base + index % across * wide, wide)
            if first:
                acc[span, put] = term
            else:
                acc[span, put] += term

        loop(total // high * across, tile)

    def turn():
        size = 128
        half = dk // 2

        def tile(index):
            for p in range(2):
                inner = aligned(index * size, size)
                span = aligned(p * rows + index * size, size)
                cos, sin = cosine[inner, :], sine[inner, :]
                for head in range(local):
                    for base, ref, scale in ((0, query, None), (half_q, keys, dk ** (-0.5))):
                        at = head * dk
                        one = acc[span, base + at : base + at + half]
                        two = acc[span, base + at + half : base + at + dk]
                        low, top = one * cos - two * sin, two * cos + one * sin
                        if scale is not None:
                            low, top = low * scale, top * scale
                        ref[span, at : at + half] = low.astype(bf16)
                        ref[span, at + half : at + dk] = top.astype(bf16)

        loop(rows // size, tile)

    strip = min(256, rows)

    def score(p, head):
        rate = rates[pl.ds(first_head + head, 1), 0:1]
        lanes = slice(head * dk, (head + 1) * dk)
        for block in range(rows // strip):
            seen = (block + 1) * strip
            q_part = query[p * rows + block * strip : p * rows + seen, lanes]
            k_part = keys[p * rows : p * rows + seen, lanes]
            product = lax.dot_general(
                q_part, k_part, (((1,), (1,)), ((), ())), preferred_element_type=f32
            )
            offset = (
                lax.broadcasted_iota(jnp.int32, (strip, seen), 0)
                - lax.broadcasted_iota(jnp.int32, (strip, seen), 1)
                + block * strip
            )
            decay = jnp.exp(rate * jnp.maximum(offset, 0).astype(f32))
            decay = jnp.where(offset >= 0, decay, 0.0)
            scores[p * local + head, block * strip : seen, :seen] = (product * decay).astype(bf16)

    def take_values():
        size = 128

        def tile(index):
            span = aligned(index * size, size)
            values[span, :] = acc[span, w_qk.shape[1] :].astype(bf16)

        loop(total // size, tile)

    def retain_head(p, head):
        gain = head_gain[pl.ds(first_head + head, 1), :]
        lanes = slice(head * dv, (head + 1) * dv)
        for block in range(rows // strip):
            seen = (block + 1) * strip
            got = mm(
                scores[p * local + head, block * strip : seen, :seen],
                values[p * rows : p * rows + seen, lanes],
            )
            mean = jnp.sum(got * got, axis=-1, keepdims=True) / dv
            scale = lax.rsqrt(mean + HEAD_EPS)
            hidden[p * rows + block * strip : p * rows + seen, lanes] = (
                got * scale * gain
            ).astype(bf16)

    high = min(256, total)

    def mine(origin):
        return origin // per_half == c

    def lane(origin):
        return aligned(origin % per_half * share, share)

    def core_copy(plane):
        first = 2 * plane % per_half
        return pltpu.make_async_remote_copy(
            src_ref=core_out.at[pl.ds(first, 2)], dst_ref=core_in.at[pl.ds(first, 2)],
            send_sem=core_send.at[first // 2], recv_sem=core_recv.at[first // 2],
            device_id=sibling, device_id_type=MESH,
        )

    def chip_copy(plane):
        first = 2 * plane % per_half
        return pltpu.make_async_remote_copy(
            src_ref=chip_out.at[pl.ds(first, 2)], dst_ref=chip_in.at[pl.ds(first, 2)],
            send_sem=chip_send.at[first // 2], recv_sem=chip_recv.at[first // 2],
            device_id=partner, device_id_type=MESH,
        )

    def middle_copy(plane):
        spot = middle.at[pl.ds(2 * plane, 2)]
        return pltpu.make_async_remote_copy(
            src_ref=spot, dst_ref=spot, send_sem=mid_send.at[plane], recv_sem=mid_recv.at[plane],
            device_id=sibling, device_id_type=MESH,
        )

    def product(ref, origin, keep, start=0, size=None):
        def tile(index):
            span = aligned(start + index * high, high)
            term = mm(hidden[span, :], ref[origin])
            if keep:
                acc[span, lane(origin)] = term
            else:
                core_out[origin % per_half, span, :] = term.astype(bf16)

        loop((total if size is None else size) // high, tile)

    def mix_partial(plane):
        @pl.when(mine(2 * plane))
        def _():
            for pick in range(2):
                product(w_out, 2 * plane + pick, True)

        @pl.when(jnp.logical_not(mine(2 * plane)))
        def _():
            for pick in range(2):
                product(w_out, 2 * plane + pick, False)
            core_copy(plane).start()

    def mix_combine(plane):
        @pl.when(mine(2 * plane))
        def _():
            core_copy(plane).wait_recv()
            for pick in range(2):
                origin = 2 * plane + pick

                def tile(index, origin=origin):
                    span = aligned(index * high, high)
                    chip_out[origin % per_half, span, :] = (
                        acc[span, lane(origin)] + core_in[origin % per_half, span, :].astype(f32)
                    ).astype(bf16)

                loop(total // high, tile)
            chip_copy(plane).start()

    def mix_finish(plane):
        @pl.when(mine(2 * plane))
        def _():
            chip_copy(plane).wait_recv()
            for pick in range(2):
                origin = 2 * plane + pick
                for p in range(2):

                    def tile(index, origin=origin, p=p):
                        inner = aligned(index * high, high)
                        span = aligned(p * rows + index * high, high)
                        at = origin % per_half
                        mixed = chip_out[at, span, :].astype(f32) + chip_in[at, span, :].astype(f32)
                        middle[origin, span, :] = (
                            raw[p, c, inner, lane(origin)].astype(f32) + mixed
                        ).astype(bf16)

                    loop(rows // high, tile)
            middle_copy(plane).start()

    def mix_settle(plane):
        @pl.when(jnp.logical_not(mine(2 * plane)))
        def _():
            middle_copy(plane).wait_recv()

    def norm_second():
        size = 64

        def tile(index):
            span = aligned(index * size, size)
            strips = [middle[origin, span, :].astype(f32) for origin in range(count)]
            mean = sum(jnp.sum(s * s, axis=-1, keepdims=True) for s in strips) / full
            scale = lax.rsqrt(mean + EPS)
            for origin in range(count):
                lanes = slice(origin * share, (origin + 1) * share)
                normed[span, lanes] = (strips[origin] * scale * chan_gain[:, lanes]).astype(bf16)

        loop(total // size, tile)

    def upward():
        wide = min(512, w_up.shape[1])
        across = w_up.shape[1] // wide

        def tile(index):
            span = aligned(index // across * high, high)
            lanes = aligned(index % across * wide, wide)
            got = jnp.maximum(mm(normed[span, :], w_up[:, lanes]), 0.0)
            hidden[span, lanes] = (got * got).astype(bf16)

        loop(total // high * across, tile)

    def end_core_copy(origin, pick):
        at = origin % per_half
        span = aligned((1 - y if pick == 0 else y) * rows, rows)
        return pltpu.make_async_remote_copy(
            src_ref=core_out.at[at, span], dst_ref=core_in.at[at, span],
            send_sem=end_core_send.at[at, pick], recv_sem=end_core_recv.at[at, pick],
            device_id=sibling, device_id_type=MESH,
        )

    def end_copy(origin):
        at = origin % per_half
        return pltpu.make_async_remote_copy(
            src_ref=last_out.at[at], dst_ref=last_in.at[at],
            send_sem=end_send.at[at], recv_sem=end_recv.at[at],
            device_id=partner, device_id_type=MESH,
        )

    def result_copy(origin):
        at = origin % per_half
        return pltpu.make_async_copy(
            values.at[aligned(at // 2 * rows, rows), aligned(at % 2 * share, share)],
            result.at[:, lane(origin)],
            result_sem.at[at],
        )

    def end_partial(origin):
        @pl.when(mine(origin))
        def _():
            product(w_down, origin, True, (1 - y) * rows, rows)

        @pl.when(jnp.logical_not(mine(origin)))
        def _():
            for pick in range(2):
                product(w_down, origin, False, (1 - y if pick == 0 else y) * rows, rows)
                end_core_copy(origin, pick).start()

    def end_combine(origin):
        @pl.when(mine(origin))
        def _():
            end_core_copy(origin, 0).wait_recv()
            at = origin % per_half

            def tile(index):
                span = aligned((1 - y) * rows + index * high, high)
                last_out[at, aligned(index * high, high), :] = (
                    acc[span, lane(origin)] + core_in[at, span, :].astype(f32)
                ).astype(bf16)

            loop(rows // high, tile)
            end_copy(origin).start()
            product(w_down, origin, True, y * rows, rows)

    def end_finish(origin):
        @pl.when(mine(origin))
        def _():
            end_core_copy(origin, 1).wait_recv()
            end_copy(origin).wait_recv()
            at = origin % per_half

            def tile(index):
                inner = aligned(index * high, high)
                span = aligned(y * rows + index * high, high)
                added = acc[span, lane(origin)] + core_in[at, span, :].astype(f32)
                added = added + last_in[at, inner, :].astype(f32)
                put = aligned(at // 2 * rows + index * high, high)
                values[put, aligned(at % 2 * share, share)] = (
                    middle[origin, span, :].astype(f32) + added
                ).astype(bf16)

            loop(rows // high, tile)
            result_copy(origin).start()

    begin_local(QK)
    own_tokens.start()
    for index in range(len(tables)):
        table_copy(index).start()
    barrier = pltpu.get_barrier_semaphore()
    for other in (partner, twin, sibling):
        pl.semaphore_signal(barrier, inc=1, device_id=other, device_id_type=MESH)

    @pl.when(z < planes - 1)
    def _():
        pl.semaphore_signal(barrier, inc=1, device_id={"fs": place + 2}, device_id_type=MESH)

    @pl.when(z > 0)
    def _():
        pl.semaphore_signal(barrier, inc=1, device_id={"fs": place - 2}, device_id_type=MESH)

    pl.semaphore_wait(
        barrier, 3 + jnp.where(z < planes - 1, 1, 0) + jnp.where(z > 0, 1, 0)
    )
    begin_pair(QK, x)
    begin_line(QK)
    own_tokens.wait()
    token_copy(0).start()
    token_copy(1).start()
    begin_pair(QK, 1 - x)
    begin_local(VV)
    begin_pair(VV, x)
    begin_pair(VV, 1 - x)
    pair_line(QK)

    def own_pair(kind, task):
        def first():
            task(piece_origin(z, 0))

        def second():
            pair_wait(kind, 1 - x)
            task(piece_origin(z, 1))

        return first, second

    def chunk(kind, step, order, task):
        def run():
            arrived(kind, step, order)
            task(piece_origin(far[step], order))

        return run

    slots = planes - 1
    span = 2 * slots
    plan = {}

    def at(slot, *tasks):
        plan.setdefault(slot, []).extend(tasks)

    def start_tokens():
        token_copy(1).wait_recv()
        token_copy(2).start()

    def first_norm():
        for index in range(len(tables)):
            table_copy(index).wait()
        token_copy(0).wait_recv()
        token_copy(2).wait_recv()
        norm_first()

    last = KINDS * span - 1
    at(4, start_tokens)
    at(5, first_norm)
    own_qk = own_pair(QK, lambda o: accumulate(QK, o, False))
    at(6, lambda: accumulate(QK, piece_origin(z, 0), True), own_qk[1])
    own_v = own_pair(VV, lambda o: accumulate(VV, o, False))
    at(10, lambda: accumulate(VV, piece_origin(z, 0), True), own_v[1])
    for number in range(span):
        step, order = number // 2, number % 2
        at(
            max(number + LAG, 7 + number // 2),
            chunk(QK, step, order, lambda o: accumulate(QK, o, False)),
        )
        at(
            max(number + span + LAG, 10 + number // 2),
            chunk(VV, step, order, lambda o: accumulate(VV, o, False)),
        )
    at(10, turn)
    for p in range(2):
        for head in range(local):
            at(11 + p, functools.partial(score, p, head))
    at(2 * span + LAG - 1, take_values)
    for p in range(2):
        for head in range(local):
            at(2 * span + LAG - 1 + p, functools.partial(retain_head, p, head))
    base = 2 * span + LAG

    def ready(kind, step):
        def run():
            if step < 0:
                pair_wait(kind, 1 - x)
            else:
                for order in range(2):
                    arrived(kind, step, order)

        return run

    def plane_of(step):
        return z if step < 0 else far[step]

    at(base, ready(OUT, -1), lambda: mix_partial(z))
    at(base + 1, lambda: mix_combine(z))
    for step in range(slots):
        when = max(2 * span + 2 * step + 1 + LAG, base + 1)
        at(when, ready(OUT, step), functools.partial(mix_partial, far[step]))
        at(when + 1, functools.partial(mix_combine, far[step]))
    for number in range(planes):
        plane = plane_of(number - 1)
        at(base + 4 + 2 * number, functools.partial(mix_finish, plane))
        at(base + 5 + 2 * number, functools.partial(mix_settle, plane))
    finish = base + 5 + 2 * (planes - 1)

    def third_norm():
        for step in range(-1, slots):
            plane = plane_of(step)

            @pl.when(jnp.logical_not(mine(2 * plane)))
            def _(plane=plane):
                core_copy(plane).wait_send()

        norm_second()

    at(finish, third_norm)

    def up_all():
        for step in range(-1, slots):
            ready(UP, step)()
        upward()

    at(finish + 1, up_all)
    chunks = [piece_origin(z, 0), piece_origin(z, 1)]
    for step in range(slots):
        chunks += [piece_origin(far[step], order) for order in range(2)]

    def down_ready(number):
        def run():
            if number > 1:
                arrived(DOWN, (number - 2) // 2, number % 2)

        return run

    for number in range(count):
        when = finish + 2 + number // 3
        arrive = 4 * span + (number - 2) + LAG
        when = min(max(when, arrive), last + 1)
        when = when if number < count - 1 else last + 2
        at(when, down_ready(number), functools.partial(end_partial, chunks[number]))
        at(when, functools.partial(end_combine, chunks[number]))
    for number in range(count):
        early = number < count // 2
        at(last + 1 if early else last + 3, functools.partial(end_finish, chunks[number]))

    def run_plan(slot):
        for task in plan.pop(slot, ()):
            task()

    for kind in range(KINDS):
        for step in range(slots):
            for order in range(2):
                if step == slots - 1 and order == 1 and kind + 1 < KINDS:
                    begin_line(kind + 1)
                service(kind, step, order)
                if step == slots - 1 and order == 1 and kind + 1 < KINDS:
                    pair_line(kind + 1)
                if step == 0 and order == 0 and kind + 2 < KINDS:
                    begin_local(kind + 2)
                    begin_pair(kind + 2, x)
                    begin_pair(kind + 2, 1 - x)
                run_plan(kind * span + 2 * step + order)
    for slot in sorted(plan):
        run_plan(slot)
    for kind in range(KINDS):
        for sub in range(len(subs[kind])):
            for part in range(2):
                pair_copy(kind, part, sub).wait_send()
        for order in range(2):

            @pl.when(z < planes - 1)
            def _(kind=kind, order=order):
                line_copy(kind, z, order, 0, place + 2).wait_send()

            @pl.when(z > 0)
            def _(kind=kind, order=order):
                line_copy(kind, z, order, 1, place - 2).wait_send()

        for step in range(slots):
            going, target = forward_way(far[step])
            for order in range(2):

                @pl.when(going)
                def _(kind=kind, order=order, step=step, target=target):
                    line_copy(kind, far[step], order, 0, target).wait_send()

                entire = whole(kind, far[step], order)
                if entire is None:
                    cross_copy(kind, far[step], order, x).wait_send()
                else:

                    @pl.when(jnp.logical_not(entire))
                    def _(kind=kind, order=order, step=step):
                        cross_copy(kind, far[step], order, x).wait_send()

                    @pl.when(entire & going)
                    def _(step=step, target=target):
                        whole_copy(far[step], 0, target).wait_send()

    @pl.when(z == 0)
    def _():
        whole_copy(z, 0, place + 2).wait_send()

    @pl.when(z == planes - 1)
    def _():
        whole_copy(z, 1, place - 2).wait_send()

    for index in range(3):
        token_copy(index).wait_send()
    for plane in range(planes):

        @pl.when(mine(2 * plane))
        def _(plane=plane):
            chip_copy(plane).wait_send()
            middle_copy(plane).wait_send()

    for origin in range(count):

        @pl.when(mine(origin))
        def _(origin=origin):
            end_copy(origin).wait_send()
            result_copy(origin).wait()

        @pl.when(jnp.logical_not(mine(origin)))
        def _(origin=origin):
            for pick in range(2):
                end_core_copy(origin, pick).wait_send()


def fused_layer(
    count, tokens, mix_gain, query_w, key_w, value_w, head_gain, out_w, chan_gain, up_w, down_w
):
    rows, width = tokens.shape
    total, full = 2 * rows, 2 * width
    planes = count // 2
    per_half = count // 2
    share = full // count
    q_cols = query_w.shape[1] // 2
    v_cols = value_w.shape[1] // 2
    ff_cols = up_w.shape[1] // 2
    local = q_cols // DK
    half = DK // 2
    spots = np.arange(rows, dtype=np.float32)
    inverse = np.float32(THETA) ** (-np.arange(half, dtype=np.float32) / np.float32(half))
    angles = spots[:, None] * inverse.astype(np.float32)
    heads = np.arange(head_gain.shape[0], dtype=np.float32)
    rate = np.log1p(-np.exp2(np.float32(-5.0) - heads)).astype(np.float32)
    rate = np.repeat(rate[:, None], 128, axis=1)
    bf16, f32 = jnp.bfloat16, jnp.float32
    dma = pltpu.SemaphoreType.DMA
    vmem = pltpu.VMEM
    scratch = [
        vmem((full, 2 * q_cols), bf16), vmem((full, v_cols), bf16),
        vmem((count, v_cols, share), bf16), vmem((full, ff_cols), bf16),
        vmem((count, ff_cols, share), bf16),
        vmem((2, 2, rows, width), bf16), vmem((total, full), bf16),
        vmem((total, 2 * q_cols + v_cols), f32),
        vmem((total, q_cols), bf16), vmem((total, q_cols), bf16), vmem((total, v_cols), bf16),
        vmem((2 * local, rows, rows), bf16), vmem((total, v_cols), bf16),
        vmem((per_half, total, share), bf16), vmem((per_half, total, share), bf16),
        vmem((per_half, total, share), bf16), vmem((per_half, total, share), bf16),
        vmem((count, total, share), bf16),
        vmem((per_half, rows, share), bf16), vmem((per_half, rows, share), bf16),
        vmem((1, full), f32), vmem((1, full), f32), vmem(head_gain.shape, f32),
        vmem((rows, half), f32), vmem((rows, half), f32), vmem(rate.shape, f32),
        dma((KINDS, planes, 2, 2)), dma((KINDS, planes, 2)), dma((planes, 2)), dma((planes,)),
        dma((KINDS, planes, 2)), dma((KINDS, planes, 2)),
        dma((KINDS, 2, 2)), dma((KINDS, 2, 2)), dma((KINDS, 2)),
        dma((3,)), dma((3,)), dma, dma((6,)),
        dma((planes // 2,)), dma((planes // 2,)), dma((planes // 2,)), dma((planes // 2,)),
        dma((planes,)), dma((planes,)),
        dma((per_half, 2)), dma((per_half, 2)), dma((per_half,)), dma((per_half,)),
        dma((per_half,)),
    ]
    return pl.pallas_call(
        functools.partial(fused_kernel, count),
        out_shape=jax.ShapeDtypeStruct((rows, width), bf16),
        in_specs=[pl.BlockSpec(memory_space=pl.ANY)] * 13,
        out_specs=pl.BlockSpec(memory_space=pl.ANY),
        scratch_shapes=scratch,
        compiler_params=pltpu.CompilerParams(
            collective_id=0, has_side_effects=True, vmem_limit_bytes=67_043_328
        ),
        name="fused_layer",
    )(
        tokens, query_w, key_w, value_w, out_w, up_w, down_w,
        mix_gain.reshape(1, full), chan_gain.reshape(1, full), head_gain,
        jnp.asarray(np.cos(angles)), jnp.asarray(np.sin(angles)), jnp.asarray(rate),
    )


def solution(mesh):
    placed = (
        P(("rep", "fs"), "tp"),
        P(),
        P("fs", "tp"),
        P("fs", "tp"),
        P("fs", "tp"),
        P(),
        P("tp", "fs"),
        P(),
        P("fs", "tp"),
        P("tp", "fs"),
    )
    parts, tps, count = mesh.shape["rep"], mesh.shape["tp"], mesh.shape["fs"]

    def body(*blocks):
        heads = blocks[2].shape[1] // DK
        if parts == 2 and tps == 2 and count % 4 == 0 and heads % 2 == 0:
            return fused_layer(count, *blocks)
        return shards(*blocks)

    return jax.shard_map(
        body, mesh=mesh, in_specs=placed, out_specs=P(("rep", "fs"), "tp"), check_vma=False
    )
```

```python
import functools

import jax
import jax.numpy as jnp
import numpy as np
from jax import lax
from jax.experimental import pallas as pl
from jax.experimental.pallas import tpu as pltpu
from jax.sharding import PartitionSpec as P


DK = 256
DV = 512
BLOCK = 128


EPS = 1e-06
HEAD_EPS = 0.05
THETA = 10000.0


def norm_rows(rows, gain):
    values = rows.astype(jnp.float32)
    scale = lax.rsqrt(jnp.mean(values * values, axis=-1, keepdims=True) + EPS)
    return (values * scale * gain).astype(jnp.bfloat16)


def rotate(field, places):
    half = field.shape[-1] // 2
    inverse = THETA ** (-jnp.arange(half, dtype=jnp.float32) / half)
    angles = places[:, None] * inverse
    cosine = jnp.cos(angles)[:, None, :]
    sine = jnp.sin(angles)[:, None, :]
    first = field[..., :half]
    second = field[..., half:]
    return jnp.concatenate(
        [first * cosine - second * sine, second * cosine + first * sine], axis=-1
    )


def retain(query, keys, values, log_rate):
    count = query.shape[0] // BLOCK
    q_blocks = query.reshape(count, BLOCK, query.shape[1])
    k_blocks = keys.reshape(count, BLOCK, keys.shape[1])
    v_blocks = values.reshape(count, BLOCK, values.shape[1])
    place = jnp.arange(BLOCK, dtype=jnp.float32)
    offset = place[:, None] - place[None, :]
    mask = jnp.where(offset >= 0, jnp.exp(log_rate * jnp.maximum(offset, 0.0)), 0.0)
    q_decay = jnp.exp(log_rate * (place + 1.0))
    k_decay = jnp.exp(log_rate * (BLOCK - 1.0 - place))
    block_decay = jnp.exp(log_rate * BLOCK)

    def advance(state, item):
        q_part, k_part, v_part = item
        scores = jnp.dot(q_part, k_part.T, preferred_element_type=jnp.float32)
        weights = (scores * mask).astype(jnp.bfloat16)
        result = jnp.dot(weights, v_part, preferred_element_type=jnp.float32)
        q_scaled = (q_part.astype(jnp.float32) * q_decay[:, None]).astype(jnp.bfloat16)
        result = result + jnp.dot(
            q_scaled, state.astype(jnp.bfloat16), preferred_element_type=jnp.float32
        )
        k_scaled = (k_part.astype(jnp.float32) * k_decay[:, None]).astype(jnp.bfloat16)
        state = state * block_decay + jnp.dot(
            k_scaled.T, v_part, preferred_element_type=jnp.float32
        )
        return (state, result)

    start = jnp.zeros((query.shape[1], values.shape[1]), jnp.float32)
    _, outputs = lax.scan(advance, start, (q_blocks, k_blocks, v_blocks))
    return outputs.reshape(count * BLOCK, values.shape[1])


def shards(tokens, mix_gain, query_w, key_w, value_w, head_gain, out_w, chan_gain, up_w, down_w):
    rows = tokens.shape[0]
    local = query_w.shape[1] // DK
    whole = lax.all_gather(tokens, "tp", axis=1, tiled=True)
    normed = norm_rows(whole, mix_gain)
    pieces = (
        lax.all_gather(query_w, "fs", axis=0, tiled=True),
        lax.all_gather(key_w, "fs", axis=0, tiled=True),
        lax.all_gather(value_w, "fs", axis=0, tiled=True),
    )
    inputs = normed
    qraw, kraw, vraw = tuple(
        (jnp.dot(inputs, piece, preferred_element_type=jnp.float32) for piece in pieces)
    )
    places = jnp.arange(rows, dtype=jnp.int32).astype(jnp.float32)
    query = rotate(qraw.reshape(rows, local, DK), places).astype(jnp.bfloat16)
    keys = (rotate(kraw.reshape(rows, local, DK), places) * DK ** (-0.5)).astype(jnp.bfloat16)
    values = vraw.reshape(rows, local, DV).astype(jnp.bfloat16)
    first_head = lax.axis_index("tp") * local
    heads = (first_head + jnp.arange(local, dtype=jnp.int32)).astype(jnp.float32)
    log_rate = jnp.log1p(-jnp.exp2(-5.0 - heads))
    retained = jax.vmap(retain, in_axes=(1, 1, 1, 0), out_axes=1)(query, keys, values, log_rate)
    gains = lax.dynamic_slice_in_dim(head_gain, first_head, local, 0)
    scale = lax.rsqrt(jnp.mean(retained * retained, axis=-1, keepdims=True) + HEAD_EPS)
    head_out = (retained * scale * gains).astype(jnp.bfloat16).reshape(rows, local * DV)
    mixer_terms = jnp.dot(
        head_out,
        lax.all_gather(out_w, "fs", axis=1, tiled=True),
        preferred_element_type=jnp.float32,
    )
    mixed = lax.psum_scatter(
        mixer_terms.astype(jnp.bfloat16), "tp", scatter_dimension=1, tiled=True
    ).astype(jnp.float32)
    middle = (tokens.astype(jnp.float32) + mixed).astype(jnp.bfloat16)
    whole_middle = lax.all_gather(middle, "tp", axis=1, tiled=True)
    chan_normed = norm_rows(whole_middle, chan_gain)
    inputs = chan_normed
    upward = jnp.dot(
        inputs, lax.all_gather(up_w, "fs", axis=0, tiled=True), preferred_element_type=jnp.float32
    )
    hidden = jnp.square(jax.nn.relu(upward)).astype(jnp.bfloat16)
    chan_terms = jnp.dot(
        hidden, lax.all_gather(down_w, "fs", axis=1, tiled=True), preferred_element_type=jnp.float32
    )
    channel = lax.psum_scatter(
        chan_terms.astype(jnp.bfloat16), "tp", scatter_dimension=1, tiled=True
    ).astype(jnp.float32)
    return (middle.astype(jnp.float32) + channel).astype(jnp.bfloat16)


MESH = pl.DeviceIdType.MESH
QK, VV, OUT, UP, DOWN = range(5)
KINDS = 5
LAG = 2


def loop(count, body):
    def step(index, carry):
        body(index)
        return carry

    lax.fori_loop(0, count, step, 0)


def aligned(start, size):
    return pl.ds(pl.multiple_of(start, size), size)


def mm(left, right):
    return jnp.dot(left, right, preferred_element_type=jnp.float32)


def fused_kernel(count, *refs):
    (
        tokens, query_w, key_w, value_w, out_w, up_w, down_w,
        mix_gain_in, chan_gain_in, head_gain_in, cosine_in, sine_in, rate_in,
        result,
        w_qk, w_v, w_out, w_up, w_down,
        raw, normed, acc, query, keys, values, scores, hidden,
        core_out, core_in, chip_out, chip_in, middle, last_out, last_in,
        mix_gain, chan_gain, head_gain, cosine, sine, rates,
        line_send, line_recv, whole_send, whole_recv, cross_send, cross_recv, pair_send, pair_recv, local_sem,
        token_send, token_recv, token_local, table_sem,
        core_send, core_recv, chip_send, chip_recv, mid_send, mid_recv,
        end_core_send, end_core_recv, end_send, end_recv, result_sem,
    ) = refs
    bf16, f32 = jnp.bfloat16, jnp.float32
    rows, width = tokens.shape
    planes = count // 2
    total = 2 * rows
    full = 2 * width
    share = full // count
    per_half = count // 2
    dk, dv = DK, DV
    local = query_w.shape[1] // dk // 2
    place = lax.axis_index("fs")
    z, y = place // 2, place % 2
    x = lax.axis_index("rep")
    c = lax.axis_index("tp")
    partner = {"fs": 2 * z + 1 - y}
    twin = {"rep": 1 - x}
    sibling = {"tp": 1 - c}
    first_head = (2 * c + y) * local

    weights = (w_qk, w_v, w_out, w_up, w_down)
    by_rows = (True, True, False, True, False)
    half_q = query_w.shape[1] // 2
    subs = (
        ((query_w, 0, half_q), (key_w, half_q, half_q)),
        ((value_w, 0, value_w.shape[1] // 2),),
        ((out_w, 0, 0),),
        ((up_w, 0, up_w.shape[1] // 2),),
        ((down_w, 0, 0),),
    )

    def region(kind, origin, part):
        ref = weights[kind]
        if by_rows[kind]:
            size = ref.shape[0] // count // 2
            return ref.at[aligned(origin * (2 * size) + part * size, size), :]
        size = ref.shape[1] // 2
        return ref.at[origin, aligned(part * size, size), :]

    def piece_origin(plane, order):
        return 2 * plane + (y if order == 0 else 1 - y)

    def own_copy(kind, sub):
        source, offset, size = subs[kind][sub]
        ref = weights[kind]
        if by_rows[kind]:
            span = source.shape[0]
            return pltpu.make_async_copy(
                source.at[:, aligned(y * size, size)],
                ref.at[aligned(place * span, span), pl.ds(offset, size)],
                local_sem.at[kind, sub],
            )
        span = source.shape[0] // 2
        return pltpu.make_async_copy(
            source.at[aligned(y * span, span), :], ref.at[place], local_sem.at[kind, sub]
        )

    def pair_copy(kind, part, sub):
        source, offset, size = subs[kind][sub]
        ref = weights[kind]
        if by_rows[kind]:
            span = source.shape[0] // 2
            src = source.at[aligned(part * span, span), aligned((1 - y) * size, size)]
            dst = ref.at[aligned(place * (2 * span) + part * span, span), pl.ds(offset, size)]
        else:
            span = source.shape[0] // 4
            src = source.at[aligned((1 - y) * (2 * span) + part * span, span), :]
            dst = ref.at[place, aligned(part * span, span), :]
        return pltpu.make_async_remote_copy(
            src_ref=src, dst_ref=dst,
            send_sem=pair_send.at[kind, part, sub], recv_sem=pair_recv.at[kind, part, sub],
            device_id=partner, device_id_type=MESH,
        )

    def pair_wait(kind, part):
        for sub in range(len(subs[kind])):
            pair_copy(kind, part, sub).wait_recv()

    def line_copy(kind, plane, order, slot, target):
        spot = region(kind, piece_origin(plane, order), x)
        return pltpu.make_async_remote_copy(
            src_ref=spot, dst_ref=spot,
            send_sem=line_send.at[kind, plane, order, slot],
            recv_sem=line_recv.at[kind, plane, order],
            device_id={"fs": target}, device_id_type=MESH,
        )

    def cross_copy(kind, plane, order, part):
        spot = region(kind, piece_origin(plane, order), part)
        return pltpu.make_async_remote_copy(
            src_ref=spot, dst_ref=spot,
            send_sem=cross_send.at[kind, plane, order],
            recv_sem=cross_recv.at[kind, plane, order],
            device_id=twin, device_id_type=MESH,
        )

    def whole(kind, plane, order):
        if (kind, order) != (DOWN, 1):
            return None
        return (plane == 0) | (plane == planes - 1)

    def whole_copy(plane, slot, target):
        spot = region(DOWN, piece_origin(plane, 1), 1 - x)
        return pltpu.make_async_remote_copy(
            src_ref=spot, dst_ref=spot,
            send_sem=whole_send.at[plane, slot], recv_sem=whole_recv.at[plane],
            device_id={"fs": target}, device_id_type=MESH,
        )

    orders = [
        sorted(range(planes), key=lambda p: (abs(p - here), (p < here) == (2 * here < planes)))[1:]
        for here in range(planes)
    ]

    def plane_at(step):
        found = jnp.int32(0)
        for here in range(planes):
            found = jnp.where(z == here, jnp.int32(orders[here][step]), found)
        return found

    far = [plane_at(step) for step in range(planes - 1)]

    def forward_way(plane):
        way = jnp.where(plane < z, 1, -1)
        ahead = z + way
        return (ahead >= 0) & (ahead < planes), place + 2 * way

    def send_own(kind, order):
        @pl.when(z < planes - 1)
        def _():
            line_copy(kind, z, order, 0, place + 2).start()

        @pl.when(z > 0)
        def _():
            line_copy(kind, z, order, 1, place - 2).start()

    def begin_local(kind):
        for sub in range(len(subs[kind])):
            own_copy(kind, sub).start()

    def begin_line(kind):
        for sub in range(len(subs[kind])):
            own_copy(kind, sub).wait()
        send_own(kind, 0)

    def begin_pair(kind, part):
        for sub in range(len(subs[kind])):
            pair_copy(kind, part, sub).start()

    def pair_line(kind):
        pair_wait(kind, x)
        send_own(kind, 1)
        if whole(kind, z, 1) is not None:
            pair_wait(kind, 1 - x)

            @pl.when(z == 0)
            def _():
                whole_copy(z, 0, place + 2).start()

            @pl.when(z == planes - 1)
            def _():
                whole_copy(z, 1, place - 2).start()

    def service(kind, step, order):
        plane = far[step]
        line_copy(kind, plane, order, 0, place).wait_recv()
        going, target = forward_way(plane)

        @pl.when(going)
        def _():
            line_copy(kind, plane, order, 0, target).start()

        entire = whole(kind, plane, order)
        if entire is None:
            cross_copy(kind, plane, order, x).start()
            return

        @pl.when(jnp.logical_not(entire))
        def _():
            cross_copy(kind, plane, order, x).start()

        @pl.when(entire & going)
        def _():
            whole_copy(plane, 0, place).wait_recv()
            whole_copy(plane, 0, target).start()

    def arrived(kind, step, order):
        plane = far[step]
        entire = whole(kind, plane, order)
        if entire is None:
            cross_copy(kind, plane, order, 1 - x).wait_recv()
            return

        @pl.when(jnp.logical_not(entire))
        def _():
            cross_copy(kind, plane, order, 1 - x).wait_recv()

        @pl.when(entire & jnp.logical_not(forward_way(plane)[0]))
        def _():
            whole_copy(plane, 0, place).wait_recv()

    def token_copy(index):
        own = raw.at[y, c]
        if index == 0:
            spot, target = own, sibling
        elif index == 1:
            spot, target = own, partner
        else:
            spot, target = raw.at[1 - y, c], sibling
        return pltpu.make_async_remote_copy(
            src_ref=spot, dst_ref=spot, send_sem=token_send.at[index],
            recv_sem=token_recv.at[index], device_id=target, device_id_type=MESH,
        )

    tables = (
        (mix_gain_in, mix_gain), (chan_gain_in, chan_gain), (head_gain_in, head_gain),
        (cosine_in, cosine), (sine_in, sine), (rate_in, rates),
    )

    def table_copy(index):
        return pltpu.make_async_copy(tables[index][0], tables[index][1], table_sem.at[index])

    own_tokens = pltpu.make_async_copy(tokens, raw.at[y, c], token_local)

    def norm_first():
        size = 64

        def tile(index):
            for p in range(2):
                span = aligned(index * size, size)
                left = raw[p, 0, span, :].astype(f32)
                right = raw[p, 1, span, :].astype(f32)
                mean = (
                    jnp.sum(left * left, axis=-1, keepdims=True)
                    + jnp.sum(right * right, axis=-1, keepdims=True)
                ) / full
                scale = lax.rsqrt(mean + EPS)
                put = aligned(p * rows + index * size, size)
                normed[put, :width] = (left * scale * mix_gain[:, :width]).astype(bf16)
                normed[put, width:] = (right * scale * mix_gain[:, width:]).astype(bf16)

        loop(rows // size, tile)

    def accumulate(kind, origin, first):
        ref = weights[kind]
        base = 0 if kind == QK else w_qk.shape[1]
        high, wide = min(256, total), min(512, ref.shape[1])
        across = ref.shape[1] // wide

        def tile(index):
            span = aligned(index // across * high, high)
            right = ref[aligned(origin * share, share), aligned(index % across * wide, wide)]
            term = mm(normed[span, aligned(origin * share, share)], right)
            put = aligned(base + index % across * wide, wide)
            if first:
                acc[span, put] = term
            else:
                acc[span, put] += term

        loop(total // high * across, tile)

    def turn():
        size = 128
        half = dk // 2

        def tile(index):
            for p in range(2):
                inner = aligned(index * size, size)
                span = aligned(p * rows + index * size, size)
                cos, sin = cosine[inner, :], sine[inner, :]
                for head in range(local):
                    for base, ref, scale in ((0, query, None), (half_q, keys, dk ** (-0.5))):
                        at = head * dk
                        one = acc[span, base + at : base + at + half]
                        two = acc[span, base + at + half : base + at + dk]
                        low, top = one * cos - two * sin, two * cos + one * sin
                        if scale is not None:
                            low, top = low * scale, top * scale
                        ref[span, at : at + half] = low.astype(bf16)
                        ref[span, at + half : at + dk] = top.astype(bf16)

        loop(rows // size, tile)

    strip = min(256, rows)

    def score(p, head):
        rate = rates[pl.ds(first_head + head, 1), 0:1]
        lanes = slice(head * dk, (head + 1) * dk)
        for block in range(rows // strip):
            seen = (block + 1) * strip
            q_part = query[p * rows + block * strip : p * rows + seen, lanes]
            k_part = keys[p * rows : p * rows + seen, lanes]
            product = lax.dot_general(
                q_part, k_part, (((1,), (1,)), ((), ())), preferred_element_type=f32
            )
            offset = (
                lax.broadcasted_iota(jnp.int32, (strip, seen), 0)
                - lax.broadcasted_iota(jnp.int32, (strip, seen), 1)
                + block * strip
            )
            decay = jnp.exp(rate * jnp.maximum(offset, 0).astype(f32))
            decay = jnp.where(offset >= 0, decay, 0.0)
            scores[p * local + head, block * strip : seen, :seen] = (product * decay).astype(bf16)

    def take_values():
        size = 128

        def tile(index):
            span = aligned(index * size, size)
            values[span, :] = acc[span, w_qk.shape[1] :].astype(bf16)

        loop(total // size, tile)

    def retain_head(p, head):
        gain = head_gain[pl.ds(first_head + head, 1), :]
        lanes = slice(head * dv, (head + 1) * dv)
        for block in range(rows // strip):
            seen = (block + 1) * strip
            got = mm(
                scores[p * local + head, block * strip : seen, :seen],
                values[p * rows : p * rows + seen, lanes],
            )
            mean = jnp.sum(got * got, axis=-1, keepdims=True) / dv
            scale = lax.rsqrt(mean + HEAD_EPS)
            hidden[p * rows + block * strip : p * rows + seen, lanes] = (
                got * scale * gain
            ).astype(bf16)

    high = min(256, total)

    def mine(origin):
        return origin // per_half == c

    def lane(origin):
        return aligned(origin % per_half * share, share)

    def core_copy(plane):
        first = 2 * plane % per_half
        return pltpu.make_async_remote_copy(
            src_ref=core_out.at[pl.ds(first, 2)], dst_ref=core_in.at[pl.ds(first, 2)],
            send_sem=core_send.at[first // 2], recv_sem=core_recv.at[first // 2],
            device_id=sibling, device_id_type=MESH,
        )

    def chip_copy(plane):
        first = 2 * plane % per_half
        return pltpu.make_async_remote_copy(
            src_ref=chip_out.at[pl.ds(first, 2)], dst_ref=chip_in.at[pl.ds(first, 2)],
            send_sem=chip_send.at[first // 2], recv_sem=chip_recv.at[first // 2],
            device_id=partner, device_id_type=MESH,
        )

    def middle_copy(plane):
        spot = middle.at[pl.ds(2 * plane, 2)]
        return pltpu.make_async_remote_copy(
            src_ref=spot, dst_ref=spot, send_sem=mid_send.at[plane], recv_sem=mid_recv.at[plane],
            device_id=sibling, device_id_type=MESH,
        )

    def product(ref, origin, keep, start=0, size=None):
        def tile(index):
            span = aligned(start + index * high, high)
            term = mm(hidden[span, :], ref[origin])
            if keep:
                acc[span, lane(origin)] = term
            else:
                core_out[origin % per_half, span, :] = term.astype(bf16)

        loop((total if size is None else size) // high, tile)

    def mix_partial(plane):
        @pl.when(mine(2 * plane))
        def _():
            for pick in range(2):
                product(w_out, 2 * plane + pick, True)

        @pl.when(jnp.logical_not(mine(2 * plane)))
        def _():
            for pick in range(2):
                product(w_out, 2 * plane + pick, False)
            core_copy(plane).start()

    def mix_combine(plane):
        @pl.when(mine(2 * plane))
        def _():
            core_copy(plane).wait_recv()
            for pick in range(2):
                origin = 2 * plane + pick

                def tile(index, origin=origin):
                    span = aligned(index * high, high)
                    chip_out[origin % per_half, span, :] = (
                        acc[span, lane(origin)] + core_in[origin % per_half, span, :].astype(f32)
                    ).astype(bf16)

                loop(total // high, tile)
            chip_copy(plane).start()

    def mix_finish(plane):
        @pl.when(mine(2 * plane))
        def _():
            chip_copy(plane).wait_recv()
            for pick in range(2):
                origin = 2 * plane + pick
                for p in range(2):

                    def tile(index, origin=origin, p=p):
                        inner = aligned(index * high, high)
                        span = aligned(p * rows + index * high, high)
                        at = origin % per_half
                        mixed = chip_out[at, span, :].astype(f32) + chip_in[at, span, :].astype(f32)
                        middle[origin, span, :] = (
                            raw[p, c, inner, lane(origin)].astype(f32) + mixed
                        ).astype(bf16)

                    loop(rows // high, tile)
            middle_copy(plane).start()

    def mix_settle(plane):
        @pl.when(jnp.logical_not(mine(2 * plane)))
        def _():
            middle_copy(plane).wait_recv()

    def norm_second():
        size = 64

        def tile(index):
            span = aligned(index * size, size)
            strips = [middle[origin, span, :].astype(f32) for origin in range(count)]
            mean = sum(jnp.sum(s * s, axis=-1, keepdims=True) for s in strips) / full
            scale = lax.rsqrt(mean + EPS)
            for origin in range(count):
                lanes = slice(origin * share, (origin + 1) * share)
                normed[span, lanes] = (strips[origin] * scale * chan_gain[:, lanes]).astype(bf16)

        loop(total // size, tile)

    def upward():
        wide = min(512, w_up.shape[1])
        across = w_up.shape[1] // wide

        def tile(index):
            span = aligned(index // across * high, high)
            lanes = aligned(index % across * wide, wide)
            got = jnp.maximum(mm(normed[span, :], w_up[:, lanes]), 0.0)
            hidden[span, lanes] = (got * got).astype(bf16)

        loop(total // high * across, tile)

    def end_core_copy(origin, pick):
        at = origin % per_half
        span = aligned((1 - y if pick == 0 else y) * rows, rows)
        return pltpu.make_async_remote_copy(
            src_ref=core_out.at[at, span], dst_ref=core_in.at[at, span],
            send_sem=end_core_send.at[at, pick], recv_sem=end_core_recv.at[at, pick],
            device_id=sibling, device_id_type=MESH,
        )

    def end_copy(origin):
        at = origin % per_half
        return pltpu.make_async_remote_copy(
            src_ref=last_out.at[at], dst_ref=last_in.at[at],
            send_sem=end_send.at[at], recv_sem=end_recv.at[at],
            device_id=partner, device_id_type=MESH,
        )

    def result_copy(origin):
        at = origin % per_half
        return pltpu.make_async_copy(
            values.at[aligned(at // 2 * rows, rows), aligned(at % 2 * share, share)],
            result.at[:, lane(origin)],
            result_sem.at[at],
        )

    def end_push(origin, pick):
        start = (1 - y if pick == 0 else y) * rows

        @pl.when(mine(origin))
        def _():
            product(w_down, origin, True, start, rows)

        @pl.when(jnp.logical_not(mine(origin)))
        def _():
            product(w_down, origin, False, start, rows)
            end_core_copy(origin, pick).start()

    def end_combine(origin):
        @pl.when(mine(origin))
        def _():
            end_core_copy(origin, 0).wait_recv()
            at = origin % per_half

            def tile(index):
                span = aligned((1 - y) * rows + index * high, high)
                last_out[at, aligned(index * high, high), :] = (
                    acc[span, lane(origin)] + core_in[at, span, :].astype(f32)
                ).astype(bf16)

            loop(rows // high, tile)
            end_copy(origin).start()

    def end_finish(origin):
        @pl.when(mine(origin))
        def _():
            end_core_copy(origin, 1).wait_recv()
            end_copy(origin).wait_recv()
            at = origin % per_half

            def tile(index):
                inner = aligned(index * high, high)
                span = aligned(y * rows + index * high, high)
                added = acc[span, lane(origin)] + core_in[at, span, :].astype(f32)
                added = added + last_in[at, inner, :].astype(f32)
                put = aligned(at // 2 * rows + index * high, high)
                values[put, aligned(at % 2 * share, share)] = (
                    middle[origin, span, :].astype(f32) + added
                ).astype(bf16)

            loop(rows // high, tile)
            result_copy(origin).start()

    begin_local(QK)
    own_tokens.start()
    for index in range(len(tables)):
        table_copy(index).start()
    barrier = pltpu.get_barrier_semaphore()
    for other in (partner, twin, sibling):
        pl.semaphore_signal(barrier, inc=1, device_id=other, device_id_type=MESH)

    @pl.when(z < planes - 1)
    def _():
        pl.semaphore_signal(barrier, inc=1, device_id={"fs": place + 2}, device_id_type=MESH)

    @pl.when(z > 0)
    def _():
        pl.semaphore_signal(barrier, inc=1, device_id={"fs": place - 2}, device_id_type=MESH)

    pl.semaphore_wait(
        barrier, 3 + jnp.where(z < planes - 1, 1, 0) + jnp.where(z > 0, 1, 0)
    )
    begin_pair(QK, x)
    begin_line(QK)
    own_tokens.wait()
    token_copy(0).start()
    token_copy(1).start()
    begin_pair(QK, 1 - x)
    begin_local(VV)
    begin_pair(VV, x)
    begin_pair(VV, 1 - x)
    pair_line(QK)

    def own_pair(kind, task):
        def first():
            task(piece_origin(z, 0))

        def second():
            pair_wait(kind, 1 - x)
            task(piece_origin(z, 1))

        return first, second

    def chunk(kind, step, order, task):
        def run():
            arrived(kind, step, order)
            task(piece_origin(far[step], order))

        return run

    slots = planes - 1
    span = 2 * slots
    plan = {}

    def at(slot, *tasks):
        plan.setdefault(slot, []).extend(tasks)

    def start_tokens():
        token_copy(1).wait_recv()
        token_copy(2).start()

    def first_norm():
        for index in range(len(tables)):
            table_copy(index).wait()
        token_copy(0).wait_recv()
        token_copy(2).wait_recv()
        norm_first()

    last = KINDS * span - 1
    at(4, start_tokens)
    at(5, first_norm)
    own_qk = own_pair(QK, lambda o: accumulate(QK, o, False))
    at(6, lambda: accumulate(QK, piece_origin(z, 0), True), own_qk[1])
    own_v = own_pair(VV, lambda o: accumulate(VV, o, False))
    at(10, lambda: accumulate(VV, piece_origin(z, 0), True), own_v[1])
    for number in range(span):
        step, order = number // 2, number % 2
        at(
            max(number + LAG, 7 + number // 2),
            chunk(QK, step, order, lambda o: accumulate(QK, o, False)),
        )
        at(
            max(number + span + LAG, 10 + number // 2),
            chunk(VV, step, order, lambda o: accumulate(VV, o, False)),
        )
    at(10, turn)
    for p in range(2):
        for head in range(local):
            at(11 + p, functools.partial(score, p, head))
    at(2 * span + LAG - 1, take_values)
    for p in range(2):
        for head in range(local):
            at(2 * span + LAG - 1 + p, functools.partial(retain_head, p, head))
    base = 2 * span + LAG

    def ready(kind, step):
        def run():
            if step < 0:
                pair_wait(kind, 1 - x)
            else:
                for order in range(2):
                    arrived(kind, step, order)

        return run

    def plane_of(step):
        return z if step < 0 else far[step]

    at(base, ready(OUT, -1), lambda: mix_partial(z))
    at(base, lambda: mix_combine(z))
    for step in range(slots):
        when = max(2 * span + 2 * step + 1 + LAG, base + 1)
        at(when, ready(OUT, step), functools.partial(mix_partial, far[step]))
        at(when + 1, functools.partial(mix_combine, far[step]))
    for number in range(planes):
        plane = plane_of(number - 1)
        at(base + 4 + 2 * number, functools.partial(mix_finish, plane))
        settle = base + 5 + 2 * number if number < planes - 1 else base + 4 + 2 * number
        at(settle, functools.partial(mix_settle, plane))
    finish = base + 4 + 2 * (planes - 1)

    def third_norm():
        for step in range(-1, slots):
            plane = plane_of(step)

            @pl.when(jnp.logical_not(mine(2 * plane)))
            def _(plane=plane):
                core_copy(plane).wait_send()

        norm_second()

    at(finish, third_norm)

    def up_all():
        for step in range(-1, slots):
            ready(UP, step)()
        upward()

    at(finish + 1, up_all)
    chunks = [piece_origin(z, 0), piece_origin(z, 1)]
    for step in range(slots):
        chunks += [piece_origin(far[step], order) for order in range(2)]

    def down_ready(number):
        def run():
            if number > 1:
                arrived(DOWN, (number - 2) // 2, number % 2)

        return run

    for number in range(count):
        when = finish + 2 + number // 3
        arrive = 4 * span + (number - 2) + LAG
        when = min(max(when, arrive), last + 1)
        if number < count - 2:
            chunk_at = chunks[number]
            at(when, down_ready(number), functools.partial(end_push, chunk_at, 0))
            at(when, functools.partial(end_combine, chunk_at))
            at(when, functools.partial(end_push, chunk_at, 1))

    def close(task, *numbers, tail=()):
        for number in numbers:
            at(last + 1, functools.partial(task, chunks[number], *tail))

    near, final = count - 2, count - 1
    close(end_finish, *range(count // 2))
    at(last + 1, down_ready(final))
    close(end_push, final, tail=(0,))
    at(last + 1, down_ready(near))
    close(end_push, near, tail=(0,))
    close(end_combine, final)
    close(end_combine, near)
    close(end_push, final, tail=(1,))
    close(end_push, near, tail=(1,))
    close(end_finish, *range(count // 2, count))

    def run_plan(slot):
        for task in plan.pop(slot, ()):
            task()

    for kind in range(KINDS):
        for step in range(slots):
            for order in range(2):
                if step == slots - 1 and order == 1 and kind + 1 < KINDS:
                    begin_line(kind + 1)
                service(kind, step, order)
                if step == slots - 1 and order == 1 and kind + 1 < KINDS:
                    pair_line(kind + 1)
                if step == 0 and order == 0 and kind + 2 < KINDS:
                    begin_local(kind + 2)
                    begin_pair(kind + 2, x)
                    begin_pair(kind + 2, 1 - x)
                run_plan(kind * span + 2 * step + order)
    for slot in sorted(plan):
        run_plan(slot)
    for kind in range(KINDS):
        for sub in range(len(subs[kind])):
            for part in range(2):
                pair_copy(kind, part, sub).wait_send()
        for order in range(2):

            @pl.when(z < planes - 1)
            def _(kind=kind, order=order):
                line_copy(kind, z, order, 0, place + 2).wait_send()

            @pl.when(z > 0)
            def _(kind=kind, order=order):
                line_copy(kind, z, order, 1, place - 2).wait_send()

        for step in range(slots):
            going, target = forward_way(far[step])
            for order in range(2):

                @pl.when(going)
                def _(kind=kind, order=order, step=step, target=target):
                    line_copy(kind, far[step], order, 0, target).wait_send()

                entire = whole(kind, far[step], order)
                if entire is None:
                    cross_copy(kind, far[step], order, x).wait_send()
                else:

                    @pl.when(jnp.logical_not(entire))
                    def _(kind=kind, order=order, step=step):
                        cross_copy(kind, far[step], order, x).wait_send()

                    @pl.when(entire & going)
                    def _(step=step, target=target):
                        whole_copy(far[step], 0, target).wait_send()

    @pl.when(z == 0)
    def _():
        whole_copy(z, 0, place + 2).wait_send()

    @pl.when(z == planes - 1)
    def _():
        whole_copy(z, 1, place - 2).wait_send()

    for index in range(3):
        token_copy(index).wait_send()
    for plane in range(planes):

        @pl.when(mine(2 * plane))
        def _(plane=plane):
            chip_copy(plane).wait_send()
            middle_copy(plane).wait_send()

    for origin in range(count):

        @pl.when(mine(origin))
        def _(origin=origin):
            end_copy(origin).wait_send()
            result_copy(origin).wait()

        @pl.when(jnp.logical_not(mine(origin)))
        def _(origin=origin):
            for pick in range(2):
                end_core_copy(origin, pick).wait_send()


def fused_layer(
    count, tokens, mix_gain, query_w, key_w, value_w, head_gain, out_w, chan_gain, up_w, down_w
):
    rows, width = tokens.shape
    total, full = 2 * rows, 2 * width
    planes = count // 2
    per_half = count // 2
    share = full // count
    q_cols = query_w.shape[1] // 2
    v_cols = value_w.shape[1] // 2
    ff_cols = up_w.shape[1] // 2
    local = q_cols // DK
    half = DK // 2
    spots = np.arange(rows, dtype=np.float32)
    inverse = np.float32(THETA) ** (-np.arange(half, dtype=np.float32) / np.float32(half))
    angles = spots[:, None] * inverse.astype(np.float32)
    heads = np.arange(head_gain.shape[0], dtype=np.float32)
    rate = np.log1p(-np.exp2(np.float32(-5.0) - heads)).astype(np.float32)
    rate = np.repeat(rate[:, None], 128, axis=1)
    bf16, f32 = jnp.bfloat16, jnp.float32
    dma = pltpu.SemaphoreType.DMA
    vmem = pltpu.VMEM
    scratch = [
        vmem((full, 2 * q_cols), bf16), vmem((full, v_cols), bf16),
        vmem((count, v_cols, share), bf16), vmem((full, ff_cols), bf16),
        vmem((count, ff_cols, share), bf16),
        vmem((2, 2, rows, width), bf16), vmem((total, full), bf16),
        vmem((total, 2 * q_cols + v_cols), f32),
        vmem((total, q_cols), bf16), vmem((total, q_cols), bf16), vmem((total, v_cols), bf16),
        vmem((2 * local, rows, rows), bf16), vmem((total, v_cols), bf16),
        vmem((per_half, total, share), bf16), vmem((per_half, total, share), bf16),
        vmem((per_half, total, share), bf16), vmem((per_half, total, share), bf16),
        vmem((count, total, share), bf16),
        vmem((per_half, rows, share), bf16), vmem((per_half, rows, share), bf16),
        vmem((1, full), f32), vmem((1, full), f32), vmem(head_gain.shape, f32),
        vmem((rows, half), f32), vmem((rows, half), f32), vmem(rate.shape, f32),
        dma((KINDS, planes, 2, 2)), dma((KINDS, planes, 2)), dma((planes, 2)), dma((planes,)),
        dma((KINDS, planes, 2)), dma((KINDS, planes, 2)),
        dma((KINDS, 2, 2)), dma((KINDS, 2, 2)), dma((KINDS, 2)),
        dma((3,)), dma((3,)), dma, dma((6,)),
        dma((planes // 2,)), dma((planes // 2,)), dma((planes // 2,)), dma((planes // 2,)),
        dma((planes,)), dma((planes,)),
        dma((per_half, 2)), dma((per_half, 2)), dma((per_half,)), dma((per_half,)),
        dma((per_half,)),
    ]
    return pl.pallas_call(
        functools.partial(fused_kernel, count),
        out_shape=jax.ShapeDtypeStruct((rows, width), bf16),
        in_specs=[pl.BlockSpec(memory_space=pl.ANY)] * 13,
        out_specs=pl.BlockSpec(memory_space=pl.ANY),
        scratch_shapes=scratch,
        compiler_params=pltpu.CompilerParams(
            collective_id=0, has_side_effects=True, vmem_limit_bytes=67_043_328
        ),
        name="fused_layer",
    )(
        tokens, query_w, key_w, value_w, out_w, up_w, down_w,
        mix_gain.reshape(1, full), chan_gain.reshape(1, full), head_gain,
        jnp.asarray(np.cos(angles)), jnp.asarray(np.sin(angles)), jnp.asarray(rate),
    )


def solution(mesh):
    placed = (
        P(("rep", "fs"), "tp"),
        P(),
        P("fs", "tp"),
        P("fs", "tp"),
        P("fs", "tp"),
        P(),
        P("tp", "fs"),
        P(),
        P("fs", "tp"),
        P("tp", "fs"),
    )
    parts, tps, count = mesh.shape["rep"], mesh.shape["tp"], mesh.shape["fs"]

    def body(*blocks):
        heads = blocks[2].shape[1] // DK
        if parts == 2 and tps == 2 and count % 4 == 0 and heads % 2 == 0:
            return fused_layer(count, *blocks)
        return shards(*blocks)

    return jax.shard_map(
        body, mesh=mesh, in_specs=placed, out_specs=P(("rep", "fs"), "tp"), check_vma=False
    )
```
